512 devices in a mesh: ep: 32 (over z, core), tp: 16 (over y, x).
Axes of the slice: x: 4, y: 4, z: 16, core: 2. Of those that a mesh axis runs over, the one named last changes fastest.
Arguments:
- mixer_input: bfloat16 [8192, 1024], P('ep', 'tp'), may hold values from -6 to 6
- log_step: float32 [64], P('tp'), may hold values from -12.8 to -2.7
- decay_shift: float32 [8192, 64], P('ep', 'tp'), may hold values from -2 to 0
- input_map: bfloat16 [2, 64, 64, 16], P(None, 'tp'), may hold values from -143.10835 to 143.10835
- readout: float32 [2, 64, 16, 64], P(None, 'tp'), may hold values from -0.5 to 0.5
- mixer_weight: bfloat16 [1024, 2048], P(None, 'tp'), may hold values from -0.1875 to 0.1875
- expert_input: bfloat16 [4096, 2048], P('ep'), may hold values from -6 to 6
- norm_gain: float32 [2048], replicated, may hold values from 0.1 to 1.9
- routes: int32 [4096, 2], P('ep'), may hold values from 0 to 31, all different within a row; in each aligned block of 128 rows (0 to 127, 128 to 255, ...) at most 16 rows name the same one
- route_weight: float32 [4096, 2], P('ep'), may hold values from 0.1 to 2.5
- expert_switch_matrix: bfloat16 [32, 2048, 4096], P('ep', None, 'tp'), may hold values from -0.125 to 0.125
- up_weight: bfloat16 [32, 2048, 4096], P('ep', None, 'tp'), may hold values from -0.125 to 0.125
- down_weight: bfloat16 [32, 4096, 2048], P('ep', None, 'tp'), may hold values from -0.09375 to 0.09375
- shared_gate: bfloat16 [2048, 1024], P(None, 'tp'), may hold values from -0.125 to 0.125
- shared_up: bfloat16 [2048, 1024], P(None, 'tp'), may hold values from -0.125 to 0.125
- shared_down: bfloat16 [1024, 2048], P(None, 'tp'), may hold values from -0.1875 to 0.1875
Outputs:
- mixer_out: bfloat16 [8192, 2048], P('ep', 'tp')
- experts_out: bfloat16 [4096, 2048], P('ep', 'tp')
The draws below stay inside these ranges and needn't reach their ends.
Inputs may be any that keep to these rules, and one draw needn't show every extreme that they name: `routes`: each row names 2 different experts. In each aligned block of 128 rows (the rows of one index of ep) no expert is named by more than 16 rows, and in some block one expert is named by exactly 16 rows.
All inputs are finite; a program needn't handle non-finite values.
Results may differ from the reference program's by a relative error of at most 0.0069.
Values may be sent and summed in bfloat16 or wider, within the bound.
A program may use at most 64 MiB of HBM per device.

```python
import math
import jax
import jax.numpy as jnp
import numpy as np
from jax import lax

D = 2048
GROUPS = 64
GROUP = 16
STATE = 64
EXPERT_FF = 4096
FF = 1024
TOPK = 2
MIX_ROWS = 256
EXP_ROWS = 128
D_SSM = 1024
MIX_TOKENS = 8192
EXP_TOKENS = 4096
EXPERTS = 32
CAP = 16
N_EP = 32


def draw_steps(key):
    pick_key, fast_key, slow_key = jax.random.split(key, 3)
    quick = jax.random.randint(pick_key, (GROUPS,), 0, 2) < 1
    fast = jax.random.uniform(fast_key, (GROUPS,), jnp.float32, math.log(0.02), math.log(0.067))
    slow = jax.random.uniform(slow_key, (GROUPS,), jnp.float32, math.log(0.2), math.log(1.2)) - math.log(MIX_TOKENS)
    return jnp.where(quick, fast, slow)


def draw_log_step(key, part):
    return draw_steps(jax.random.fold_in(key, 101))


def draw_input_map(key, part):
    steps = draw_steps(jax.random.fold_in(key, 101))
    noise_key = jax.random.fold_in(key, 202)
    noise = jax.random.truncated_normal(noise_key, -4.0, 4.0, (2, GROUPS, STATE, GROUP), jnp.float32)
    scale = jnp.exp(-0.5 * steps)[None, :, None, None] / math.sqrt(2.0 * GROUP)
    return (noise * scale).astype(jnp.bfloat16)


def draw_decay_shift(key, part):
    rate_key, place_key, depth_key = jax.random.split(jax.random.fold_in(key, 303), 3)
    block_count = MIX_TOKENS // MIX_ROWS
    lowest, highest = (0.05, 0.4)
    block_rate = jnp.exp(jax.random.uniform(rate_key, (block_count, GROUPS), jnp.float32, math.log(lowest), math.log(highest))) / MIX_TOKENS
    shift_magnitude = -jnp.repeat(block_rate, MIX_ROWS, axis=0)
    capacity_indices = jax.random.randint(place_key, (2, GROUPS), 0, MIX_TOKENS)
    stack_levels = jnp.log(jax.random.uniform(depth_key, (2, GROUPS), jnp.float32, 0.55, 0.8))
    element_ordinals = jnp.arange(MIX_TOKENS, dtype=jnp.int32)[:, None, None]
    sequence_groupings = jnp.sum(jnp.where(element_ordinals == capacity_indices[None], stack_levels[None], 0.0), axis=1)
    return shift_magnitude + sequence_groupings


def steps_of(key, shape, pieces, least, high):
    def one(axis_at, blocks):
        steps = jax.random.uniform(jax.random.fold_in(jax.random.fold_in(key, 6), axis_at), (blocks,), jnp.float32, least / len(pieces), high / len(pieces))
        return jnp.repeat(jnp.exp(steps), shape[axis_at] // blocks).reshape((-1,) + (1,) * (len(shape) - axis_at - 1))

    level = one(*pieces[0])
    for cut in pieces[1:]:
        level = level * one(*cut)
    return level


def routed_block(key, own, number, rows, count, top, reach, slope):
    sequence = jax.random.permutation(key, count)
    crowded, common = load_shares(count, rows * top, reach, slope, True), load_shares(count, rows * top, reach, slope, False)
    places = jnp.arange(count)

    def named(tallies, turn):
        used = int((tallies > 0).sum())
        fixed = max(1, used // 4)
        shifted = fixed + (places - fixed + turn * (used - fixed)) % max(1, count - fixed)
        return jnp.zeros((count,), jnp.int32).at[sequence[jnp.where(places < fixed, places, shifted)]].set(jnp.asarray(tallies, jnp.int32))

    tallies = jnp.where(number % 4 == 0, named(crowded, number // 4), named(common, number - number // 4 - 1))
    mixed = jax.random.permutation(jax.random.fold_in(own, 3), count)
    donor, receiver = mixed[0:count // 2 * 2:2], mixed[1:count // 2 * 2:2]
    room = jnp.minimum(tallies[donor] - 1, reach - tallies[receiver]) // 2
    room = jnp.where((donor == sequence[0]) | (receiver == sequence[0]) | (tallies[receiver] == 0), 0, jnp.maximum(room, 0))
    shifted = jax.random.randint(jax.random.fold_in(own, 4), (count // 2,), 0, 1 << 20) % (room + 1)
    tallies = tallies.at[donor].add(-shifted).at[receiver].add(shifted)
    items = jnp.searchsorted(jnp.cumsum(tallies), jnp.arange(rows * top), side="right").astype(jnp.int32)
    table = items.reshape(top, rows).T
    table = table[jax.random.permutation(jax.random.fold_in(own, 1), rows)]
    turn = jax.random.randint(jax.random.fold_in(own, 2), (rows, 1), 0, top)
    return jnp.take_along_axis(table, (jnp.arange(top)[None, :] + turn) % top, axis=1)


def load_shares(amount, total, most, lean, full):
    weights = [(1 << 20) // math.isqrt(rank ** lean) + 1 for rank in range(1, amount + 1)]
    largest = most if full else min(most, max(-(-total // amount), total * weights[0] // sum(weights)))
    least = 1 if total - largest >= amount - 1 else 0
    holding, surplus = [largest] + [least] * (amount - 1), total - largest - least * (amount - 1)
    while surplus > 0:
        free = [i for i in range(1, amount) if holding[i] < largest] or [i for i in range(1, amount) if holding[i] < most]
        pool, remaining = sum([weights[i] for i in free]), surplus
        for i in free:
            addition = min(most - holding[i], max(1, remaining * weights[i] // pool), surplus)
            holding[i] = holding[i] + addition
            surplus = surplus - addition
    return np.array(holding)


def normal_values(key, shape, scale, bound, cuts=(), held_as=jnp.bfloat16):
    drawn = jax.random.normal(key, shape, jnp.float32) * scale
    if len(cuts) > 0:
        drawn = steps_of(key, shape, cuts, -0.22, 0.18) * drawn
    return jnp.clip(drawn, min=-bound, max=bound).astype(held_as)


def setup_inputs(seed: int = 0) -> dict:
    arg_keys = jax.random.split(jax.random.key(seed), 17)
    mixer_input = normal_values(arg_keys[0], (MIX_TOKENS, D_SSM), 1.0, 6.0, ((0, 32), (1, 16)))
    log_step = draw_log_step(jax.random.fold_in(arg_keys[16], 71), 0)
    decay_shift = draw_decay_shift(jax.random.fold_in(arg_keys[16], 71), 0)
    input_map = draw_input_map(jax.random.fold_in(arg_keys[16], 71), 0)
    readout = normal_values(arg_keys[4], (2, GROUPS, GROUP, STATE), (2 * STATE) ** -0.5, 0.5, ((1, 16),), jnp.float32)
    mixer_weight = normal_values(arg_keys[5], (D_SSM, D), D_SSM ** -0.5, 0.1875, ((1, 16),))
    expert_input = normal_values(arg_keys[6], (EXP_TOKENS, D), 1.0, 6.0, ((0, 32),))
    norm_gain = jnp.clip(1.0 + 0.18 * jax.random.normal(arg_keys[7], (D,), jnp.float32), 0.1, 1.9)
    routes_keys = jax.random.split(jax.random.fold_in(arg_keys[8], 1), EXP_TOKENS // EXP_ROWS)
    routes_turns = jax.random.permutation(jax.random.fold_in(arg_keys[8], 3), EXP_TOKENS // EXP_ROWS)
    routes = jax.vmap(lambda own, number: routed_block(jax.random.fold_in(arg_keys[8], 2), own, number, EXP_ROWS, EXPERTS, TOPK, CAP, 1))(routes_keys, routes_turns).reshape((EXP_TOKENS, TOPK))
    route_weight = jnp.clip(jnp.exp(math.log(2.5) - 3.218876 * jax.random.uniform(arg_keys[9], (EXP_TOKENS, TOPK), jnp.float32) ** steps_of(arg_keys[9], (EXP_TOKENS, TOPK), ((0, 32),), -0.2, 0.2)), 0.1, 2.5)
    expert_switch_matrix = normal_values(arg_keys[10], (EXPERTS, D, EXPERT_FF), D ** -0.5, 0.125, ((0, 32), (2, 16)))
    up_weight = normal_values(arg_keys[11], (EXPERTS, D, EXPERT_FF), D ** -0.5, 0.125, ((0, 32), (2, 16)))
    down_weight = normal_values(arg_keys[12], (EXPERTS, EXPERT_FF, D), EXPERT_FF ** -0.5, 0.09375, ((0, 32), (2, 16)))
    shared_gate = normal_values(arg_keys[13], (D, FF), D ** -0.5, 0.125, ((1, 16),))
    shared_up = normal_values(arg_keys[14], (D, FF), D ** -0.5, 0.125, ((1, 16),))
    shared_down = normal_values(arg_keys[15], (FF, D), FF ** -0.5, 0.1875, ((1, 16),))
    return {"mixer_input": mixer_input, "log_step": log_step, "decay_shift": decay_shift, "input_map": input_map, "readout": readout, "mixer_weight": mixer_weight, "expert_input": expert_input, "norm_gain": norm_gain, "routes": routes, "route_weight": route_weight, "expert_switch_matrix": expert_switch_matrix, "up_weight": up_weight, "down_weight": down_weight, "shared_gate": shared_gate, "shared_up": shared_up, "shared_down": shared_down}


def combine_parts(earlier, later):
    early_real, early_imaginary, early_shift_real, early_shift_imaginary = earlier
    late_real, late_imaginary, late_shift_real, late_shift_imaginary = later
    joint_real = late_real * early_real - late_imaginary * early_imaginary
    joint_imaginary = late_real * early_imaginary + late_imaginary * early_real
    shift_real = late_real * early_shift_real - late_imaginary * early_shift_imaginary + late_shift_real
    shift_imaginary = late_real * early_shift_imaginary + late_imaginary * early_shift_real + late_shift_imaginary
    return (joint_real, joint_imaginary, shift_real, shift_imaginary)

def factors(log_step, states):
    step_rate = jnp.exp(log_step)
    frequency = jnp.pi * jnp.arange(states, dtype=jnp.float32)
    angle = step_rate[:, None] * frequency[None, :]
    turn_cosine = jnp.cos(angle)
    turn_sine = jnp.sin(angle)
    base = jnp.exp(-0.5 * step_rate)[:, None]
    base_real = base * turn_cosine
    starting_quadrature = base * turn_sine
    inverse = 1.0 / (0.25 + frequency * frequency)[None, :]
    lowered = base_real - 1.0
    inject_real = (-0.5 * lowered + starting_quadrature * frequency[None, :]) * inverse
    inject_imaginary = (-0.5 * starting_quadrature - lowered * frequency[None, :]) * inverse
    return (step_rate, turn_cosine, turn_sine, inject_real, inject_imaginary)

def reference(mixer_input, log_step, decay_shift, input_map, readout, mixer_weight, expert_input, norm_gain, routes, route_weight, expert_switch_matrix, up_weight, down_weight, shared_gate, shared_up, shared_down):
    highest = lax.Precision.HIGHEST
    step_rate, turn_cosine, turn_sine, inject_real, inject_imaginary = factors(log_step, STATE)
    blocks_in = mixer_input.reshape(N_EP, MIX_ROWS, GROUPS, GROUP)
    blocks_shift = decay_shift.reshape(N_EP, MIX_ROWS, GROUPS)
    map_real = input_map[0].astype(jnp.float32)
    map_imaginary = input_map[1].astype(jnp.float32)

    def advance(carry, inputs):
        carry_real, carry_imaginary = carry
        block_in, block_shift = inputs
        magnitude = jnp.exp(-0.5 * step_rate[None, :] + block_shift)[:, :, None]
        decay_real = magnitude * turn_cosine[None]
        decay_imaginary = magnitude * turn_sine[None]
        values = block_in.astype(jnp.float32)
        drive_real = jnp.einsum('tgh,gph->tgp', values, map_real, precision=highest)
        drive_imaginary = jnp.einsum('tgh,gph->tgp', values, map_imaginary, precision=highest)
        push_real = inject_real[None] * drive_real - inject_imaginary[None] * drive_imaginary
        push_imaginary = inject_real[None] * drive_imaginary + inject_imaginary[None] * drive_real
        total_real, total_imaginary, local_real, local_imaginary = lax.associative_scan(combine_parts, (decay_real, decay_imaginary, push_real, push_imaginary), axis=0)
        state_real = local_real + total_real * carry_real[None] - total_imaginary * carry_imaginary[None]
        state_imaginary = local_imaginary + total_real * carry_imaginary[None] + total_imaginary * carry_real[None]
        mixed = jnp.einsum('ghp,tgp->tgh', readout[0], state_real, precision=highest) - jnp.einsum('ghp,tgp->tgh', readout[1], state_imaginary, precision=highest)
        return ((state_real[-1], state_imaginary[-1]), mixed.reshape(MIX_ROWS, GROUPS * GROUP))
    start = (jnp.zeros((GROUPS, STATE), jnp.float32), jnp.zeros((GROUPS, STATE), jnp.float32))
    _, outputs = lax.scan(advance, start, (blocks_in, blocks_shift))
    activated = jax.nn.gelu(outputs.reshape(MIX_TOKENS, GROUPS * GROUP)).astype(jnp.bfloat16)
    mixer_out = jnp.dot(activated, mixer_weight, preferred_element_type=jnp.float32).astype(jnp.bfloat16)
    values = expert_input.astype(jnp.float32)
    normed = (values * lax.rsqrt(lax.optimization_barrier(jnp.mean(values * values, axis=-1, keepdims=True)) + 1e-06) * norm_gain).astype(jnp.bfloat16)
    shared_hidden = (jax.nn.silu(jnp.dot(normed, shared_gate, preferred_element_type=jnp.float32)) * jnp.dot(normed, shared_up, preferred_element_type=jnp.float32)).astype(jnp.bfloat16)
    common_contribution = jnp.dot(shared_hidden, shared_down, preferred_element_type=jnp.float32)
    token_count = EXP_TOKENS
    limit = N_EP * CAP
    padded = jnp.concatenate([normed, jnp.zeros((1, D), jnp.bfloat16)], axis=0)

    def expert_step(total, expert):
        chosen = routes == expert
        member = jnp.any(chosen, axis=1)
        weight = lax.optimization_barrier(jnp.sum(jnp.where(chosen, route_weight, 0.0), axis=1))
        position = (jnp.cumsum(member.astype(jnp.int32)) - 1).astype(jnp.int32)
        target = jnp.where(member, position, limit).astype(jnp.int32)
        holder = jnp.full((limit,), token_count, jnp.int32).at[target].set(jnp.arange(token_count, dtype=jnp.int32), mode='drop')
        rows = padded[holder]
        hidden = (jax.nn.silu(jnp.dot(rows, expert_switch_matrix[expert], preferred_element_type=jnp.float32)) * jnp.dot(rows, up_weight[expert], preferred_element_type=jnp.float32)).astype(jnp.bfloat16)
        part = jnp.dot(hidden, down_weight[expert], preferred_element_type=jnp.float32).astype(jnp.bfloat16)
        scale = jnp.concatenate([weight, jnp.zeros((1,), jnp.float32)], axis=0)[holder]
        return (total.at[holder].add(part.astype(jnp.float32) * scale[:, None]), None)
    routed_output, _ = lax.scan(expert_step, jnp.zeros((token_count + 1, D), jnp.float32), jnp.arange(EXPERTS, dtype=jnp.int32))
    experts_out = (common_contribution + routed_output[:token_count]).astype(jnp.bfloat16)
    return (mixer_out, experts_out)
```

```python
import jax
import jax.numpy as jnp
from jax import lax
from jax.experimental import pallas as pl
from jax.experimental.pallas import tpu as pltpu
from jax.sharding import PartitionSpec as P

MESH = pl.DeviceIdType.MESH
F32 = jnp.float32
BF16 = jnp.bfloat16
HIGHEST = lax.Precision.HIGHEST

CHUNKS = 4
CHUNK = 128
CAP = 16
REACH = [0, 1, -1, 2, -4, 5, -5, 6, -6, 7, -7, 8, -2, 3, -3, 4]
SLOTS = [(dz, flip) for dz in REACH for flip in (0, 1)]
SLOT_OF = {(dz % 16, flip): k for k, (dz, flip) in enumerate(SLOTS)}


def dot(a, b, precision=None):
    return jnp.dot(a, b, preferred_element_type=F32, precision=precision)


def dot_nt(a, b, precision=None):
    return lax.dot_general(
        a, b, (((1,), (1,)), ((), ())), preferred_element_type=F32, precision=precision
    )


def iota(shape, dim):
    return lax.broadcasted_iota(jnp.int32, shape, dim)


def put(ref, at, value):
    ref[0, at, :] = value[:, :128]
    ref[1, at, :] = value[:, 128:]


def got(ref, at):
    return jnp.concatenate([ref[0, at, :], ref[1, at, :]], axis=1)


class Gather:
    def __init__(self, buf, send, recv, number, place):
        self.buf, self.send, self.recv, self.number = buf, send, recv, number
        self.ep, self.y, self.x = place
        rows = buf.shape[2]
        half, quarter = rows // 2, rows // 4
        y, x = self.y, self.x
        self.xr, self.xl = (x + 1) % 4, (x + 3) % 4
        self.yu, self.yd = (y + 1) % 4, (y + 3) % 4
        xr, xl, yu, yd = self.xr, self.xl, self.yu, self.yd
        a, b = pl.ds(0, half), pl.ds(half, half)
        a0, a1 = pl.ds(0, quarter), pl.ds(quarter, quarter)
        b0, b1 = pl.ds(half, quarter), pl.ds(half + quarter, quarter)
        right, left, up, down = (y, xr), (y, xl), (yu, x), (yd, x)
        self.plan = [
            (buf.at[y, x, a], right),
            (buf.at[y, x, a], left),
            (buf.at[y, x, b], up),
            (buf.at[y, x, b], down),
            (buf.at[y, xl, a0], right),
            (buf.at[y, xr, a1], left),
            (buf.at[yd, x, b0], up),
            (buf.at[yu, x, b1], down),
            (buf.at[y, :, a], up),
            (buf.at[y, :, a], down),
            (buf.at[:, x, b], right),
            (buf.at[:, x, b], left),
            (buf.at[yd, :, a0], up),
            (buf.at[yu, :, a1], down),
            (buf.at[:, xl, b0], right),
            (buf.at[:, xr, b1], left),
        ]

    def copy(self, m):
        ref, (y, x) = self.plan[m]
        return pltpu.make_async_remote_copy(
            src_ref=ref,
            dst_ref=ref,
            send_sem=self.send.at[self.number, m],
            recv_sem=self.recv.at[self.number, m],
            device_id=(self.ep, y * 4 + x),
            device_id_type=MESH,
        )

    def stage(self, s):
        if s == 0:
            for m in range(4):
                self.copy(m).start()
        elif s == 2 or s == 4:
            for m in range(4 * s - 4, 4 * s):
                self.copy(m).wait_recv()
            if s == 2:
                for m in range(8, 12):
                    self.copy(m).start()
        else:
            for m in range(4 * s - 4, 4 * s):
                self.copy(m).wait_recv()
                self.copy(m + 4).start()

    def finish(self):
        for m in range(16):
            self.copy(m).wait_send()


def body(
    x_ref, fac_ref, shift_ref, imap_ref, rout_ref, e_ref, gain_ref, routes_ref, rw_ref,
    mixw_hbm, wg_hbm, wu_hbm, wd_hbm, sg_hbm, su_hbm, sd_hbm,
    mix_ref, exp_ref,
    mixw, wg, wu, wd, sg, su, sd,
    normed, outgoing, sel, rows_buf, hid_buf, res, returned, m_buf, sums,
    push_r, push_i, mag, ph_r, ph_i, keep,
    load_sem, g_send, g_recv, z_send, z_recv, s_send, s_recv, r_send, r_recv,
):
    ep, tp = lax.axis_index("ep"), lax.axis_index("tp")
    z, core = ep // 2, ep % 2
    y, x = tp // 4, tp % 4

    loads = [
        pltpu.make_async_copy(src, dst, load_sem.at[k])
        for k, (src, dst) in enumerate(
            [(sg_hbm, sg), (su_hbm, su), (wg_hbm, wg), (wu_hbm, wu), (wd_hbm, wd),
             (sd_hbm, sd), (mixw_hbm, mixw)]
        )
    ]
    for load in loads:
        load.start()

    def far(dz, flip):
        return ((z + dz + 16) % 16) * 2 + (core + flip) % 2

    barrier = pltpu.get_barrier_semaphore()
    for dz, flip in SLOTS[1:]:
        pl.semaphore_signal(barrier, inc=1, device_id=(far(dz, flip), tp), device_id_type=MESH)
    for ny, nx in ((y, (x + 1) % 4), (y, (x + 3) % 4), ((y + 1) % 4, x), ((y + 3) % 4, x)):
        pl.semaphore_signal(barrier, inc=1, device_id=(ep, ny * 4 + nx), device_id_type=MESH)

    values = e_ref[...].astype(F32)
    scale = lax.rsqrt(jnp.mean(values * values, axis=-1, keepdims=True) + 1e-06)
    normed[...] = (values * scale * gain_ref[...]).astype(BF16)
    lane = iota((128, 128), 1)
    named = [(routes_ref[:, k : k + 1] == lane).astype(F32) for k in (0, 1)]
    earlier = (iota((128, 128), 0) > lane).astype(BF16)
    before = dot(earlier, (named[0] + named[1]).astype(BF16))
    wide = iota((128, 512), 1)
    for k in (0, 1):
        rank = jnp.sum(named[k] * before, axis=1, keepdims=True).astype(jnp.int32)
        sel[k] = (routes_ref[:, k : k + 1] * CAP + rank == wide).astype(BF16)
    own = normed[:, pl.ds(pl.multiple_of(tp * 128, 128), 128)]
    chosen = sel[0].astype(F32) + sel[1].astype(F32)
    outgoing[...] = lax.dot_general(
        chosen.astype(BF16), own, (((0,), (0,)), ((), ())), preferred_element_type=F32
    ).astype(BF16)

    pl.semaphore_wait(barrier, len(SLOTS) - 1 + 4)

    def block_of(k):
        return pl.ds((k % 8) * CAP, CAP)

    def row_send(k):
        dz, flip = SLOTS[k]
        there = SLOT_OF[(-dz % 16, flip)]
        expert = far(dz, flip)
        return pltpu.make_async_remote_copy(
            src_ref=outgoing.at[pl.ds(pl.multiple_of(expert * CAP, CAP), CAP)],
            dst_ref=rows_buf.at[there // 8, y, x, block_of(there)],
            send_sem=z_send,
            recv_sem=z_recv.at[there // 8],
            device_id=(expert, tp),
            device_id_type=MESH,
        )

    for k in range(1, 32):
        row_send(k).start()
    rows_buf[0, y, x, 0:CAP] = outgoing[pl.ds(pl.multiple_of(ep * CAP, CAP), CAP)]

    def rows_arrived(c):
        if c == 0:
            ref = rows_buf.at[0, y, x, pl.ds(CAP, CHUNK - CAP)]
        else:
            ref = rows_buf.at[c, y, x]
        pltpu.make_async_copy(ref, ref, z_recv.at[c]).wait()

    cosine, sine = fac_ref[0:1, :], fac_ref[1:2, :]
    inj_r, inj_i, low = fac_ref[2:3, :], fac_ref[3:4, :], fac_ref[4:5, :]
    spread = (iota((16, 64), 1) % 16 == iota((16, 64), 0)).astype(BF16)
    in_map = dot(imap_ref[...], spread)
    in_map = jnp.where((iota((512, 64), 0) // 64) % 4 == iota((512, 64), 1) // 16, in_map, 0.0)
    drive = dot_nt(x_ref[...], in_map.astype(BF16))
    drive_r, drive_i = drive[:, :256], drive[:, 256:]
    every = slice(None)
    put(push_r, every, inj_r * drive_r - inj_i * drive_i)
    put(push_i, every, inj_r * drive_i + inj_i * drive_r)
    group = iota((256, 256), 1) // 64
    shift = jnp.where(group == 0, shift_ref[:, 0:1], shift_ref[:, 1:2])
    shift = jnp.where(group == 2, shift_ref[:, 2:3], shift)
    shift = jnp.where(group == 3, shift_ref[:, 3:4], shift)
    put(mag, every, jnp.exp(low + shift))
    state_r, state_i = jnp.zeros((8, 256), F32), jnp.zeros((8, 256), F32)
    total = jnp.ones((8, 256), F32)
    turn_r, turn_i = jnp.ones((1, 256), F32), jnp.zeros((1, 256), F32)
    for j in range(32):
        at = pl.ds(j, 8, stride=32)
        m = got(mag, at)
        d_r, d_i = m * cosine, m * sine
        state_r, state_i = (
            d_r * state_r - d_i * state_i + got(push_r, at),
            d_r * state_i + d_i * state_r + got(push_i, at),
        )
        total = total * m
        turn_r, turn_i = turn_r * cosine - turn_i * sine, turn_r * sine + turn_i * cosine
        put(push_r, at, state_r)
        put(push_i, at, state_i)
        put(mag, at, total)
        ph_r[j : j + 1, :] = turn_r
        ph_i[j : j + 1, :] = turn_i
    all_r, all_i = total * turn_r, total * turn_i
    c_r, c_i = jnp.zeros((1, 256), F32), jnp.zeros((1, 256), F32)
    t_r, t_i = jnp.ones((1, 256), F32), jnp.zeros((1, 256), F32)
    for s in range(8):
        for n, part in enumerate((t_r, t_i, c_r, c_i)):
            keep[n, s : s + 1, :] = part
        a_r, a_i = all_r[s : s + 1], all_i[s : s + 1]
        c_r, c_i = (
            a_r * c_r - a_i * c_i + state_r[s : s + 1],
            a_r * c_i + a_i * c_r + state_i[s : s + 1],
        )
        t_r, t_i = a_r * t_r - a_i * t_i, a_r * t_i + a_i * t_r
    for n, part in enumerate((t_r, t_i, c_r, c_i)):
        sums[ep, 2 * n : 2 * n + 1, :] = part[:, :128]
        sums[ep, 2 * n + 1 : 2 * n + 2, :] = part[:, 128:]

    for k in range(1, 32):
        pltpu.make_async_remote_copy(
            src_ref=sums.at[ep],
            dst_ref=sums.at[ep],
            send_sem=s_send,
            recv_sem=s_recv,
            device_id=(far(*SLOTS[k]), tp),
            device_id_type=MESH,
        ).start()

    place = (ep, y, x)
    rows = [Gather(rows_buf.at[c], g_send, g_recv, c, place) for c in range(CHUNKS)]
    hid = [Gather(hid_buf.at[c], g_send, g_recv, CHUNKS + c, place) for c in range(CHUNKS)]
    both = Gather(m_buf, g_send, g_recv, 2 * CHUNKS, place)

    def packed(top, bottom):
        first = (iota((64, 128), 1) == iota((64, 128), 0)).astype(BF16)
        second = (iota((64, 128), 1) == iota((64, 128), 0) + 64).astype(BF16)
        return (dot(top, first) + dot(bottom, second)).astype(BF16)

    def silu(v):
        return v / (1.0 + jnp.exp(-v))

    def shared_part():
        loads[0].wait()
        loads[1].wait()
        hidden = (silu(dot(normed[...], sg[...])) * dot(normed[...], su[...])).astype(BF16)
        m_buf[y, x, 128:192] = packed(hidden[:64], hidden[64:])

    def mixer_part():
        pltpu.make_async_copy(sums.at[pl.ds(0, 31)], sums.at[pl.ds(0, 31)], s_recv).wait()
        in_r, in_i = jnp.zeros((2, 128), F32), jnp.zeros((2, 128), F32)
        for i in range(32):
            a_r, a_i = sums[i, 0:2, :], sums[i, 2:4, :]
            n_r = a_r * in_r - a_i * in_i + sums[i, 4:6, :]
            n_i = a_r * in_i + a_i * in_r + sums[i, 6:8, :]
            in_r, in_i = jnp.where(i < ep, n_r, in_r), jnp.where(i < ep, n_i, in_i)
        in_r = jnp.concatenate([in_r[0:1], in_r[1:2]], axis=1)
        in_i = jnp.concatenate([in_i[0:1], in_i[1:2]], axis=1)
        k_r, k_i = keep[0], keep[1]
        car_r = k_r * in_r - k_i * in_i + keep[2]
        car_i = k_r * in_i + k_i * in_r + keep[3]
        for j in range(32):
            at = pl.ds(j, 8, stride=32)
            p_r, p_i, m = ph_r[j : j + 1, :], ph_i[j : j + 1, :], got(mag, at)
            put(push_r, at, got(push_r, at) + m * (p_r * car_r - p_i * car_i))
            put(push_i, at, got(push_i, at) + m * (p_r * car_i + p_i * car_r))
        spread = (iota((64, 256), 1) % 64 == iota((64, 256), 0)).astype(F32)
        mine = iota((64, 256), 0) // 16 == iota((64, 256), 1) // 64
        out_r = jnp.where(mine, dot(rout_ref[0:64, :], spread, HIGHEST), 0.0)
        out_i = jnp.where(mine, dot(rout_ref[64:128, :], spread, HIGHEST), 0.0)
        every = slice(None)
        v = dot_nt(got(push_r, every), out_r, HIGHEST) - dot_nt(got(push_i, every), out_i, HIGHEST)
        act = 0.5 * v * (1.0 + jnp.tanh(0.7978845608 * (v + 0.044715 * v * v * v)))
        act = act.astype(BF16)
        m_buf[y, x, 0:128] = packed(act[:128], act[128:])

    def joined(ref):
        return jnp.concatenate([ref[s // 4, s % 4] for s in range(16)], axis=1)

    def up_part(c):
        if c == 0:
            loads[2].wait()
            loads[3].wait()
        piece = joined(rows_buf.at[c])
        hid_buf[c, y, x] = (silu(dot(piece, wg[...])) * dot(piece, wu[...])).astype(BF16)

    def down_part(c):
        if c == 0:
            loads[4].wait()
        res[c * CHUNK : (c + 1) * CHUNK] = dot(joined(hid_buf.at[c]), wd[...]).astype(BF16)
        home = pl.ds(pl.multiple_of(ep * CAP, CAP), CAP)
        for k in range(8 * c, 8 * c + 8):
            if k == 0:
                returned[home] = res[0:CAP]
                continue
            pltpu.make_async_remote_copy(
                src_ref=res.at[pl.ds(k * CAP, CAP)],
                dst_ref=returned.at[home],
                send_sem=r_send,
                recv_sem=r_recv,
                device_id=(far(*SLOTS[k]), tp),
                device_id_type=MESH,
            ).start()

    def spread_out(start, height, weight):
        low_half = iota((height, 128), 1) < 64
        total = jnp.zeros((2 * height, 128), F32)
        for s in range(16):
            block = m_buf[s // 4, s % 4, start : start + height]
            zero = jnp.zeros_like(block)
            both_rows = jnp.concatenate(
                [jnp.where(low_half, block, zero), jnp.where(low_half, zero, block)], axis=0
            )
            w = weight[s * 64 : (s + 1) * 64]
            total += dot(both_rows, jnp.concatenate([w, w], axis=0))
        return total

    rows_arrived(0)
    rows[0].stage(0)
    shared_part()
    rows_arrived(1)
    rows[0].stage(1)
    rows[1].stage(0)
    rows_arrived(2)
    rows[0].stage(2)
    rows[1].stage(1)
    rows[2].stage(0)
    rows_arrived(3)
    rows[0].stage(3)
    rows[1].stage(2)
    rows[2].stage(1)
    rows[3].stage(0)
    mixer_part()
    both.stage(0)
    rows[0].stage(4)
    rows[1].stage(3)
    rows[2].stage(2)
    rows[3].stage(1)
    up_part(0)
    hid[0].stage(0)
    both.stage(1)
    rows[1].stage(4)
    rows[2].stage(3)
    rows[3].stage(2)
    up_part(1)
    hid[0].stage(1)
    hid[1].stage(0)
    both.stage(2)
    rows[2].stage(4)
    rows[3].stage(3)
    up_part(2)
    hid[0].stage(2)
    hid[1].stage(1)
    hid[2].stage(0)
    both.stage(3)
    rows[3].stage(4)
    up_part(3)
    hid[0].stage(3)
    hid[1].stage(2)
    hid[2].stage(1)
    hid[3].stage(0)
    both.stage(4)
    loads[5].wait()
    loads[6].wait()
    mix_ref[...] = spread_out(0, 128, mixw).astype(BF16)
    hid[0].stage(4)
    hid[1].stage(3)
    hid[2].stage(2)
    hid[3].stage(1)
    down_part(0)
    hid[1].stage(4)
    hid[2].stage(3)
    hid[3].stage(2)
    down_part(1)
    hid[2].stage(4)
    hid[3].stage(3)
    down_part(2)
    common = spread_out(128, 64, sd)
    hid[3].stage(4)
    down_part(3)

    for gather in rows + hid + [both]:
        gather.finish()
    sent = outgoing.at[pl.ds(0, 31 * CAP)]
    pltpu.make_async_copy(sent, sent, z_send).wait()
    pltpu.make_async_copy(sums.at[pl.ds(0, 31)], sums.at[pl.ds(0, 31)], s_send).wait()
    back = returned.at[pl.ds(0, 31 * CAP)]
    pltpu.make_async_copy(back, back, r_send).wait()
    pltpu.make_async_copy(back, back, r_recv).wait()
    for k in (0, 1):
        common += rw_ref[:, k : k + 1] * dot(sel[k], returned[...])
    exp_ref[...] = common.astype(BF16)


def factors(log_step, states):
    step_rate = jnp.exp(log_step)
    frequency = jnp.pi * jnp.arange(states, dtype=jnp.float32)
    angle = step_rate[:, None] * frequency[None, :]
    turn_cosine = jnp.cos(angle)
    turn_sine = jnp.sin(angle)
    base = jnp.exp(-0.5 * step_rate)[:, None]
    base_real = base * turn_cosine
    starting_quadrature = base * turn_sine
    inverse = 1.0 / (0.25 + frequency * frequency)[None, :]
    lowered = base_real - 1.0
    inject_real = (-0.5 * lowered + starting_quadrature * frequency[None, :]) * inverse
    inject_imaginary = (-0.5 * starting_quadrature - lowered * frequency[None, :]) * inverse
    low = jnp.broadcast_to(-0.5 * step_rate[:, None], angle.shape)
    none = jnp.zeros_like(angle)
    rows = (turn_cosine, turn_sine, inject_real, inject_imaginary, low, none, none, none)
    return jnp.stack([row.reshape(-1) for row in rows])


def shards(
    mixer_input, log_step, decay_shift, input_map, readout, mixer_weight, expert_input,
    norm_gain, routes, route_weight, expert_switch_matrix, up_weight, down_weight,
    shared_gate, shared_up, shared_down,
):
    vmem = pl.BlockSpec(memory_space=pltpu.VMEM)
    hbm = pl.BlockSpec(memory_space=pl.ANY)
    V, DMA = pltpu.VMEM, pltpu.SemaphoreType.DMA
    return pl.pallas_call(
        body,
        out_shape=(
            jax.ShapeDtypeStruct((256, 128), BF16),
            jax.ShapeDtypeStruct((128, 128), BF16),
        ),
        in_specs=[vmem] * 9 + [hbm] * 7,
        out_specs=(vmem, vmem),
        scratch_shapes=[
            V((1024, 128), BF16),
            V((2048, 256), BF16),
            V((2048, 256), BF16),
            V((4096, 128), BF16),
            V((2048, 64), BF16),
            V((2048, 64), BF16),
            V((1024, 128), BF16),
            V((128, 2048), BF16),
            V((512, 128), BF16),
            V((2, 128, 512), BF16),
            V((CHUNKS, 4, 4, CHUNK, 128), BF16),
            V((CHUNKS, 4, 4, CHUNK, 256), BF16),
            V((512, 128), BF16),
            V((512, 128), BF16),
            V((4, 4, 192, 128), BF16),
            V((32, 8, 128), F32),
            V((2, 256, 128), F32),
            V((2, 256, 128), F32),
            V((2, 256, 128), F32),
            V((32, 256), F32),
            V((32, 256), F32),
            V((4, 8, 256), F32),
            DMA((7,)),
            DMA((2 * CHUNKS + 1, 16)),
            DMA((2 * CHUNKS + 1, 16)),
            DMA,
            DMA((CHUNKS,)),
            DMA,
            DMA,
            DMA,
            DMA,
        ],
        compiler_params=pltpu.CompilerParams(
            collective_id=0, has_side_effects=True, vmem_limit_bytes=50 * 1024 * 1024
        ),
    )(
        mixer_input,
        factors(log_step, 64),
        decay_shift,
        input_map.reshape(512, 16),
        readout.reshape(128, 64),
        expert_input,
        norm_gain.reshape(1, 2048),
        routes,
        route_weight,
        mixer_weight,
        expert_switch_matrix[0],
        up_weight[0],
        down_weight[0],
        shared_gate,
        shared_up,
        shared_down,
    )


def solution(mesh):
    placed = (
        P("ep", "tp"),
        P("tp"),
        P("ep", "tp"),
        P(None, "tp", None, None),
        P(None, "tp", None, None),
        P(None, "tp"),
        P("ep", None),
        P(),
        P("ep", None),
        P("ep", None),
        P("ep", None, "tp"),
        P("ep", None, "tp"),
        P("ep", None, "tp"),
        P(None, "tp"),
        P(None, "tp"),
        P(None, "tp"),
    )
    return jax.shard_map(
        shards, mesh=mesh, in_specs=placed, out_specs=(P("ep", "tp"), P("ep", "tp")), check_vma=False
    )
```

```python
import jax
import jax.numpy as jnp
from jax import lax
from jax.experimental import pallas as pl
from jax.experimental.pallas import tpu as pltpu
from jax.sharding import PartitionSpec as P

MESH = pl.DeviceIdType.MESH
F32 = jnp.float32
BF16 = jnp.bfloat16
HIGHEST = lax.Precision.HIGHEST

CHUNKS = 4
CHUNK = 128
CAP = 16
REACH = [0, 1, -1, 2, -4, 5, -5, 6, -6, 7, -7, 8, -2, 3, -3, 4]
SLOTS = [(dz, flip) for dz in REACH for flip in (0, 1)]
SLOT_OF = {(dz % 16, flip): k for k, (dz, flip) in enumerate(SLOTS)}


def dot(a, b, precision=None):
    return jnp.dot(a, b, preferred_element_type=F32, precision=precision)


def dot_nt(a, b, precision=None):
    return lax.dot_general(
        a, b, (((1,), (1,)), ((), ())), preferred_element_type=F32, precision=precision
    )


def dot_tn(a, b, precision=None):
    return lax.dot_general(
        a, b, (((0,), (0,)), ((), ())), preferred_element_type=F32, precision=precision
    )


def iota(shape, dim):
    return lax.broadcasted_iota(jnp.int32, shape, dim)


def put(ref, at, value):
    ref[0, at, :] = value[:, :128]
    ref[1, at, :] = value[:, 128:]


def got(ref, at):
    return jnp.concatenate([ref[0, at, :], ref[1, at, :]], axis=1)


PASSED_ON = {0: 0, 1: 1, 2: 2, 3: 3, 4: 4, 5: 5, 6: 6, 7: 7, 8: 8, 9: 9}
PASSED_ON = {**PASSED_ON, 12: 21, 13: 22}


class Gather:
    def __init__(self, buf, send, recv, number, place):
        self.buf, self.send, self.recv, self.number = buf, send, recv, number
        self.ep, self.y, self.x = place
        self.half = buf.shape[1] // 2
        self.plan = []
        for turned in (False, True):
            messages = [(0, 0, None, 0, 1), (0, 0, None, 0, -1), (0, 0, None, 1, 1), (0, 0, None, 1, -1)]
            messages += [(-1, 0, 0, 0, 1), (1, 0, 1, 0, -1)]
            messages += [(i, 0, None, 1, d) for i in (-1, 1) for d in (1, -1)]
            messages += [(0, -1, 0, 1, 1), (0, 1, 1, 1, -1)]
            messages += [(2, 0, None, 1, 1), (2, 0, None, 1, -1)]
            messages += [(i, -d, (1 - d) // 2, 1, d) for i in (-1, 1) for d in (1, -1)]
            messages += [(2, -1, 0, 1, 1), (2, 1, 1, 1, -1)]
            self.plan += [(turned, *m) for m in messages]

    def copy(self, m):
        turned, i, j, part, ring, step = self.plan[m]
        dy, dx = (i, j) if turned else (j, i)
        shard = ((self.y + dy + 4) % 4) * 4 + (self.x + dx + 4) % 4
        start, count = (self.half if turned else 0), self.half
        if part is not None:
            count = self.half // 2
            start += part * count
        along_y = (ring == 0) == turned
        ny = (self.y + step + 4) % 4 if along_y else self.y
        nx = self.x if along_y else (self.x + step + 4) % 4
        ref = self.buf.at[shard, pl.ds(start, count)]
        stage = sum(m % 20 >= first for first in (4, 12, 18))
        arrival = PASSED_ON.get(m % 20)
        arrival = 20 if arrival is None else arrival + (2 if arrival > 20 else 10) * (m // 20)
        return pltpu.make_async_remote_copy(
            src_ref=ref,
            dst_ref=ref,
            send_sem=self.send.at[self.number, stage],
            recv_sem=self.recv.at[self.number, arrival],
            device_id=(self.ep, ny * 4 + nx),
            device_id_type=MESH,
        )

    def whole(self, count, sem):
        ref = self.buf.at[pl.ds(0, count)]
        pltpu.make_async_copy(ref, ref, sem).wait()

    def stage(self, s):
        with jax.named_scope(f"g{self.number}s{s}"):
            if s == 4:
                self.whole(4, self.recv.at[self.number, 20])
                return
            then = [
                [(None, (0, 1, 2, 3))],
                [(0, (4, 6, 7)), (1, (5, 8, 9)), (2, (10,)), (3, (11,))],
                [(4, ()), (5, (12, 13)), (6, (14,)), (7, (15,)), (8, (16,)), (9, (17,))],
                [(12, (18,)), (13, (19,))],
            ][s]
            for wait, starts in then:
                for turn in (0, 20):
                    if wait is not None:
                        self.copy(turn + wait).wait_recv()
                    for m in starts:
                        self.copy(turn + m).start()

    def finish(self):
        for stage, count in enumerate((4, 6, 4, 1)):
            self.whole(count, self.send.at[self.number, stage])


def factors(log_step, state):
    step_rate = jnp.exp(log_step)
    frequency = jnp.pi * state.astype(F32)
    angle = step_rate * frequency
    turn_cosine = jnp.cos(angle)
    turn_sine = jnp.sin(angle)
    base = jnp.exp(-0.5 * step_rate)
    base_real = base * turn_cosine
    starting_quadrature = base * turn_sine
    inverse = 1.0 / (0.25 + frequency * frequency)
    lowered = base_real - 1.0
    inject_real = (-0.5 * lowered + starting_quadrature * frequency) * inverse
    inject_imaginary = (-0.5 * starting_quadrature - lowered * frequency) * inverse
    return (turn_cosine, turn_sine, inject_real, inject_imaginary, -0.5 * step_rate)


def body(
    step_ref, x_hbm, shift_hbm, imap_hbm, rout_hbm, e_hbm, gain_hbm, routes_hbm, rw_hbm,
    mixw_hbm, wg_hbm, wu_hbm, wd_hbm, sg_hbm, su_hbm, sd_hbm,
    mix_ref, exp_ref,
    x_ref, shift_ref, imap_ref, rout_ref, e_ref, gain_ref, routes_ref, rw_ref, mixw, wg, wu, wd, sgu, sd,
    normed, outgoing, back_hi, back_lo, rows_buf, hid_buf, res, returned, mix_buf, sh_buf, pair, chips,
    push_r, push_i, mag, ph_r, ph_i, keep,
    load_sem, g_send, g_recv, z_send, z_recv, s_send, s_recv, r_send, r_recv,
):
    ep, tp = lax.axis_index("ep"), lax.axis_index("tp")
    z, core = ep // 2, ep % 2
    y, x = tp // 4, tp % 4

    loads = [
        pltpu.make_async_copy(src, dst, load_sem.at[k])
        for k, (src, dst) in enumerate(
            [(sg_hbm, sgu.at[0:64]), (su_hbm, sgu.at[64:128]), (wg_hbm, wg), (wu_hbm, wu),
             (wd_hbm, wd), (sd_hbm, sd), (mixw_hbm, mixw), (e_hbm, e_ref), (gain_hbm, gain_ref),
             (routes_hbm, routes_ref), (x_hbm, x_ref), (shift_hbm, shift_ref),
             (imap_hbm, imap_ref), (rout_hbm, rout_ref), (rw_hbm, rw_ref)]
        )
    ]
    for k in (7, 8, 9, 10, 11, 12, 13, 14, 0, 1, 2, 3, 4, 5, 6):
        loads[k].start()

    def far(dz, flip):
        return ((z + dz + 16) % 16) * 2 + (core + flip) % 2

    chips[...] = jnp.zeros_like(chips)
    barrier = pltpu.get_barrier_semaphore()
    for dz, flip in SLOTS[1:]:
        pl.semaphore_signal(barrier, inc=1, device_id=(far(dz, flip), tp), device_id_type=MESH)
    for ny, nx in ((y, (x + 1) % 4), (y, (x + 3) % 4), ((y + 1) % 4, x), ((y + 3) % 4, x)):
        pl.semaphore_signal(barrier, inc=1, device_id=(ep, ny * 4 + nx), device_id_type=MESH)

    with jax.named_scope("load"):
        for k in (7, 8, 9):
            loads[k].wait()
    values = e_ref[...].astype(F32)
    scale = lax.rsqrt(jnp.mean(values * values, axis=-1, keepdims=True) + 1e-06)
    normed[...] = (values * scale * gain_ref[...]).astype(BF16)
    expert = iota((32, 128), 0)
    named = [(routes_ref[k : k + 1, :] == expert).astype(F32) for k in (0, 1)]
    earlier = (iota((128, 128), 0) < iota((128, 128), 1)).astype(BF16)
    before = dot((named[0] + named[1]).astype(BF16), earlier)
    slot = iota((512, 128), 0)
    took = []
    for k in (0, 1):
        rank = jnp.sum(named[k] * before, axis=0, keepdims=True).astype(jnp.int32)
        took.append((routes_ref[k : k + 1, :] * CAP + rank == slot).astype(F32))
    own = normed[:, pl.ds(pl.multiple_of(tp * 128, 128), 128)]
    outgoing[...] = dot((took[0] + took[1]).astype(BF16), own).astype(BF16)

    with jax.named_scope("enter"):
        pl.semaphore_wait(barrier, len(SLOTS) - 1 + 4)

    def block_of(k):
        return pl.ds((k % 8) * CAP, CAP)

    def row_send(k):
        dz, flip = SLOTS[k]
        there = SLOT_OF[(-dz % 16, flip)]
        expert = far(dz, flip)
        return pltpu.make_async_remote_copy(
            src_ref=outgoing.at[pl.ds(pl.multiple_of(expert * CAP, CAP), CAP)],
            dst_ref=rows_buf.at[there // 8, tp, block_of(there)],
            send_sem=z_send,
            recv_sem=z_recv.at[there // 8],
            device_id=(expert, tp),
            device_id_type=MESH,
        )

    def send_chunk(c):
        for k in range(1, 32):
            dz, flip = SLOTS[k]
            if SLOT_OF[(-dz % 16, flip)] // 8 == c:
                row_send(k).start()

    send_chunk(0)
    rows_buf[0, tp, 0:CAP] = outgoing[pl.ds(pl.multiple_of(ep * CAP, CAP), CAP)]

    def rows_arrived(c):
        if c == 0:
            ref = rows_buf.at[0, tp, pl.ds(CAP, CHUNK - CAP)]
        else:
            ref = rows_buf.at[c, tp]
        pltpu.make_async_copy(ref, ref, z_recv.at[c]).wait()

    def to_partner():
        return pltpu.make_async_remote_copy(
            src_ref=pair.at[core],
            dst_ref=pair.at[core],
            send_sem=s_send.at[0],
            recv_sem=s_recv.at[0],
            device_id=(far(0, 1), tp),
            device_id_type=MESH,
        )

    def to_chip(dz):
        return pltpu.make_async_remote_copy(
            src_ref=chips.at[z],
            dst_ref=chips.at[z],
            send_sem=s_send.at[dz],
            recv_sem=s_recv.at[dz],
            device_id=(far(dz, 0), tp),
            device_id_type=MESH,
        )

    def parts_of(ref, i):
        return [ref[i, 2 * n : 2 * n + 2, :] for n in range(4)]

    def after(early_r, early_i, late):
        a_r, a_i, c_r, c_i = late
        return a_r * early_r - a_i * early_i + c_r, a_r * early_i + a_i * early_r + c_i

    def pair_part():
        to_partner().wait_recv()
        first, second = parts_of(pair, 0), parts_of(pair, 1)
        a_r, a_i = first[0] * second[0] - first[1] * second[1], first[0] * second[1] + first[1] * second[0]
        c_r, c_i = after(first[2], first[3], second)
        for n, part in enumerate((a_r, a_i, c_r, c_i)):
            chips[z, 2 * n : 2 * n + 2, :] = part
        for dz in range(1, 16):

            @pl.when(z + dz < 16)
            def _(dz=dz):
                to_chip(dz).start()

    def scan_part():
        with jax.named_scope("load2"):
            for k in (10, 11, 12):
                loads[k].wait()
        group = iota((1, 256), 1) // 64
        log_step = jnp.where(group == 0, step_ref[0], step_ref[1])
        log_step = jnp.where(group == 2, step_ref[2], log_step)
        log_step = jnp.where(group == 3, step_ref[3], log_step)
        cosine, sine, inj_r, inj_i, low = factors(log_step, iota((1, 256), 1) % 64)
        spread = (iota((64, 256), 1) % 64 == iota((64, 256), 0)).astype(BF16)
        mine = iota((64, 256), 0) // 16 == iota((64, 256), 1) // 64
        drive_r, drive_i = [
            dot_tn(
                x_ref[...],
                jnp.where(mine, dot(imap_ref[64 * c : 64 * c + 64, :], spread), 0.0).astype(BF16),
            )
            for c in (0, 1)
        ]
        every = slice(None)
        put(push_r, every, inj_r * drive_r - inj_i * drive_i)
        put(push_i, every, inj_r * drive_i + inj_i * drive_r)
        of_group = (iota((4, 256), 1) // 64 == iota((4, 256), 0)).astype(F32)
        put(mag, every, jnp.exp(low + dot_tn(shift_ref[...], of_group, HIGHEST)))
        state_r, state_i = jnp.zeros((8, 256), F32), jnp.zeros((8, 256), F32)
        total = jnp.ones((8, 256), F32)
        turn_r, turn_i = jnp.ones((1, 256), F32), jnp.zeros((1, 256), F32)
        for j in range(32):
            at = pl.ds(j, 8, stride=32)
            m = got(mag, at)
            d_r, d_i = m * cosine, m * sine
            state_r, state_i = (
                d_r * state_r - d_i * state_i + got(push_r, at),
                d_r * state_i + d_i * state_r + got(push_i, at),
            )
            total = total * m
            turn_r, turn_i = turn_r * cosine - turn_i * sine, turn_r * sine + turn_i * cosine
            put(push_r, at, state_r)
            put(push_i, at, state_i)
            put(mag, at, total)
            ph_r[j : j + 1, :] = turn_r
            ph_i[j : j + 1, :] = turn_i
        all_r, all_i = total * turn_r, total * turn_i
        c_r, c_i = jnp.zeros((1, 256), F32), jnp.zeros((1, 256), F32)
        t_r, t_i = jnp.ones((1, 256), F32), jnp.zeros((1, 256), F32)
        for s in range(8):
            for n, part in enumerate((t_r, t_i, c_r, c_i)):
                keep[n, s : s + 1, :] = part
            a_r, a_i = all_r[s : s + 1], all_i[s : s + 1]
            c_r, c_i = (
                a_r * c_r - a_i * c_i + state_r[s : s + 1],
                a_r * c_i + a_i * c_r + state_i[s : s + 1],
            )
            t_r, t_i = a_r * t_r - a_i * t_i, a_r * t_i + a_i * t_r
        for n, part in enumerate((t_r, t_i, c_r, c_i)):
            pair[core, 2 * n : 2 * n + 1, :] = part[:, :128]
            pair[core, 2 * n + 1 : 2 * n + 2, :] = part[:, 128:]
        to_partner().start()

    place = (ep, y, x)
    rows = [Gather(rows_buf.at[c], g_send, g_recv, c, place) for c in range(CHUNKS)]
    hid = [Gather(hid_buf.at[c], g_send, g_recv, CHUNKS + c, place) for c in range(CHUNKS)]
    mixed = Gather(mix_buf, g_send, g_recv, 2 * CHUNKS, place)
    shared = Gather(sh_buf, g_send, g_recv, 2 * CHUNKS + 1, place)

    def packed(top, bottom):
        first = (iota((64, 128), 1) == iota((64, 128), 0)).astype(BF16)
        second = (iota((64, 128), 1) == iota((64, 128), 0) + 64).astype(BF16)
        return (dot(top, first) + dot(bottom, second)).astype(BF16)

    def silu(v):
        return v / (1.0 + jnp.exp(-v))

    def shared_part():
        loads[0].wait()
        loads[1].wait()
        both_sums = dot_nt(normed[...], sgu[...])
        hidden = (silu(both_sums[:, :64]) * both_sums[:, 64:]).astype(BF16)
        sh_buf[tp] = packed(hidden[:64], hidden[64:])

    def mixer_part():
        with jax.named_scope("sums"):
            for dz in range(1, 16):

                @pl.when(z - dz >= 0)
                def _(dz=dz):
                    to_chip(dz).wait_recv()

        in_r, in_i = jnp.zeros((2, 128), F32), jnp.zeros((2, 128), F32)
        for i in range(15):
            n_r, n_i = after(in_r, in_i, parts_of(chips, i))
            in_r, in_i = jnp.where(i < z, n_r, in_r), jnp.where(i < z, n_i, in_i)
        n_r, n_i = after(in_r, in_i, parts_of(pair, 0))
        in_r, in_i = jnp.where(core == 1, n_r, in_r), jnp.where(core == 1, n_i, in_i)
        in_r = jnp.concatenate([in_r[0:1], in_r[1:2]], axis=1)
        in_i = jnp.concatenate([in_i[0:1], in_i[1:2]], axis=1)
        k_r, k_i = keep[0], keep[1]
        car_r = k_r * in_r - k_i * in_i + keep[2]
        car_i = k_r * in_i + k_i * in_r + keep[3]
        for j in range(32):
            at = pl.ds(j, 8, stride=32)
            p_r, p_i, m = ph_r[j : j + 1, :], ph_i[j : j + 1, :], got(mag, at)
            put(push_r, at, got(push_r, at) + m * (p_r * car_r - p_i * car_i))
            put(push_i, at, got(push_i, at) + m * (p_r * car_i + p_i * car_r))
        loads[13].wait()
        spread = (iota((64, 256), 1) % 64 == iota((64, 256), 0)).astype(F32)
        mine = iota((64, 256), 0) // 16 == iota((64, 256), 1) // 64
        out_r = jnp.where(mine, dot(rout_ref[0:64, :], spread, HIGHEST), 0.0)
        out_i = jnp.where(mine, dot(rout_ref[64:128, :], spread, HIGHEST), 0.0)
        every = slice(None)
        v = dot_nt(got(push_r, every), out_r, HIGHEST) - dot_nt(got(push_i, every), out_i, HIGHEST)
        act = 0.5 * v * (1.0 + jnp.tanh(0.7978845608 * (v + 0.044715 * v * v * v)))
        act = act.astype(BF16)
        mix_buf[tp] = packed(act[:128], act[128:])

    def joined(ref):
        return jnp.concatenate([ref[s] for s in range(16)], axis=1)

    def up_part(c):
        if c == 0:
            loads[2].wait()
            loads[3].wait()
        piece = joined(rows_buf.at[c])
        hid_buf[c, tp] = (silu(dot(piece, wg[...])) * dot(piece, wu[...])).astype(BF16)

    def down_part(c):
        if c == 0:
            loads[4].wait()
        res[c * CHUNK : (c + 1) * CHUNK] = dot(joined(hid_buf.at[c]), wd[...]).astype(BF16)
        home = pl.ds(pl.multiple_of(ep * CAP, CAP), CAP)
        for k in range(8 * c, 8 * c + 8):
            if k == 0:
                returned[home] = res[0:CAP]
                continue
            pltpu.make_async_remote_copy(
                src_ref=res.at[pl.ds(k * CAP, CAP)],
                dst_ref=returned.at[home],
                send_sem=r_send,
                recv_sem=r_recv,
                device_id=(far(*SLOTS[k]), tp),
                device_id_type=MESH,
            ).start()

    def spread_out(buf, weight):
        height = buf.shape[1]
        low_half = iota((height, 128), 1) < 64
        total = jnp.zeros((2 * height, 128), F32)
        for s in range(16):
            block = buf[s]
            zero = jnp.zeros_like(block)
            both_rows = jnp.concatenate(
                [jnp.where(low_half, block, zero), jnp.where(low_half, zero, block)], axis=0
            )
            w = weight[s * 64 : (s + 1) * 64]
            total += dot(both_rows, jnp.concatenate([w, w], axis=0))
        return total

    def arrive(c):
        with jax.named_scope(f"arrive{c}"):
            rows_arrived(c)
        rows[c].stage(0)

    def up(c):
        rows[c].stage(4)
        with jax.named_scope(f"up{c}"):
            up_part(c)
        hid[c].stage(0)

    def down(c):
        with jax.named_scope(f"down{c}"):
            down_part(c)

    with jax.named_scope("shared_part"):
        shared_part()
    arrive(0)
    for c in (1, 2, 3):
        send_chunk(c)
    shared.stage(0)
    with jax.named_scope("scan"):
        scan_part()
    rows[0].stage(1)
    shared.stage(1)
    loads[14].wait()
    weighted = jnp.transpose(took[0] * rw_ref[0:1, :] + took[1] * rw_ref[1:2, :])
    rounded = weighted.astype(BF16)
    back_hi[...] = rounded
    back_lo[...] = (weighted - rounded.astype(F32)).astype(BF16)
    with jax.named_scope("pair"):
        pair_part()
    rows[0].stage(2)
    shared.stage(2)
    arrive(1)
    rows[0].stage(3)
    shared.stage(3)
    arrive(2)
    rows[1].stage(1)
    up(0)
    shared.stage(4)
    arrive(3)
    rows[2].stage(1)
    rows[1].stage(2)
    hid[0].stage(1)
    with jax.named_scope("mixer_part"):
        mixer_part()
    mixed.stage(0)
    rows[3].stage(1)
    rows[2].stage(2)
    rows[1].stage(3)
    hid[0].stage(2)
    mixed.stage(1)
    up(1)
    rows[2].stage(3)
    rows[3].stage(2)
    hid[0].stage(3)
    mixed.stage(2)
    up(2)
    rows[3].stage(3)
    hid[1].stage(1)
    hid[0].stage(4)
    mixed.stage(3)
    up(3)
    hid[1].stage(2)
    hid[2].stage(1)
    down(0)
    mixed.stage(4)
    hid[1].stage(3)
    hid[2].stage(2)
    hid[3].stage(1)
    loads[5].wait()
    loads[6].wait()
    mix_ref[...] = spread_out(mix_buf, mixw).astype(BF16)
    hid[1].stage(4)
    hid[2].stage(3)
    hid[3].stage(2)
    down(1)
    hid[2].stage(4)
    hid[3].stage(3)
    down(2)
    common = spread_out(sh_buf, sd)
    hid[3].stage(4)
    down(3)

    with jax.named_scope("finish"):
        for gather in rows + hid + [mixed, shared]:
            gather.finish()
        to_partner().wait_send()
        for dz in range(1, 16):

            @pl.when(z + dz < 16)
            def _(dz=dz):
                to_chip(dz).wait_send()

    sent = outgoing.at[pl.ds(0, 31 * CAP)]
    pltpu.make_async_copy(sent, sent, z_send).wait()
    back = returned.at[pl.ds(0, 31 * CAP)]
    pltpu.make_async_copy(back, back, r_send).wait()
    with jax.named_scope("last"):
        pltpu.make_async_copy(back, back, r_recv).wait()
    common += dot(back_hi[...], returned[...]) + dot(back_lo[...], returned[...])
    exp_ref[...] = common.astype(BF16)


def shards(
    mixer_input, log_step, decay_shift, input_map, readout, mixer_weight, expert_input,
    norm_gain, routes, route_weight, expert_switch_matrix, up_weight, down_weight,
    shared_gate, shared_up, shared_down,
):
    vmem = pl.BlockSpec(memory_space=pltpu.VMEM)
    hbm = pl.BlockSpec(memory_space=pltpu.HBM)
    V, DMA = pltpu.VMEM, pltpu.SemaphoreType.DMA
    return pl.pallas_call(
        body,
        out_shape=(
            jax.ShapeDtypeStruct((256, 128), BF16),
            jax.ShapeDtypeStruct((128, 128), BF16),
        ),
        in_specs=[pl.BlockSpec(memory_space=pltpu.SMEM)] + [hbm] * 15,
        out_specs=(vmem, vmem),
        scratch_shapes=[
            V((64, 256), BF16),
            V((4, 256), F32),
            V((128, 64), BF16),
            V((128, 64), F32),
            V((128, 2048), BF16),
            V((1, 2048), F32),
            V((2, 128), jnp.int32),
            V((2, 128), F32),
            V((1024, 128), BF16),
            V((2048, 256), BF16),
            V((2048, 256), BF16),
            V((4096, 128), BF16),
            V((128, 2048), BF16),
            V((1024, 128), BF16),
            V((128, 2048), BF16),
            V((512, 128), BF16),
            V((128, 512), BF16),
            V((128, 512), BF16),
            V((CHUNKS, 16, CHUNK, 128), BF16),
            V((CHUNKS, 16, CHUNK, 256), BF16),
            V((512, 128), BF16),
            V((512, 128), BF16),
            V((16, 128, 128), BF16),
            V((16, 64, 128), BF16),
            V((2, 8, 128), F32),
            V((16, 8, 128), F32),
            V((2, 256, 128), F32),
            V((2, 256, 128), F32),
            V((2, 256, 128), F32),
            V((32, 256), F32),
            V((32, 256), F32),
            V((4, 8, 256), F32),
            DMA((15,)),
            DMA((2 * CHUNKS + 2, 4)),
            DMA((2 * CHUNKS + 2, 25)),
            DMA,
            DMA((CHUNKS,)),
            DMA((16,)),
            DMA((16,)),
            DMA,
            DMA,
        ],
        compiler_params=pltpu.CompilerParams(
            collective_id=0, has_side_effects=True, vmem_limit_bytes=67_043_328
        ),
    )(
        log_step,
        mixer_input.T,
        decay_shift.T,
        jnp.swapaxes(input_map, 2, 3).reshape(128, 64),
        readout.reshape(128, 64),
        expert_input,
        norm_gain.reshape(1, 2048),
        routes.T,
        route_weight.T,
        mixer_weight,
        expert_switch_matrix[0],
        up_weight[0],
        down_weight[0],
        shared_gate.T,
        shared_up.T,
        shared_down,
    )


def solution(mesh):
    placed = (
        P("ep", "tp"),
        P("tp"),
        P("ep", "tp"),
        P(None, "tp", None, None),
        P(None, "tp", None, None),
        P(None, "tp"),
        P("ep", None),
        P(),
        P("ep", None),
        P("ep", None),
        P("ep", None, "tp"),
        P("ep", None, "tp"),
        P("ep", None, "tp"),
        P(None, "tp"),
        P(None, "tp"),
        P(None, "tp"),
    )
    return jax.shard_map(
        shards, mesh=mesh, in_specs=placed, out_specs=(P("ep", "tp"), P("ep", "tp")), check_vma=False
    )
```

```python
import heapq

import jax
import jax.numpy as jnp
from jax import lax
from jax.experimental import pallas as pl
from jax.experimental.pallas import tpu as pltpu
from jax.sharding import PartitionSpec as P

MESH = pl.DeviceIdType.MESH
F32 = jnp.float32
BF16 = jnp.bfloat16
HIGHEST = lax.Precision.HIGHEST

CHUNKS = 4
CHUNK = 128
CAP = 16
REACH = [0, 1, -1, 2, -4, 5, -5, 6, -6, 7, -7, 8, -2, 3, -3, 4]
SLOTS = [(dz, flip) for dz in REACH for flip in (0, 1)]


def dot(a, b, precision=None):
    return jnp.dot(a, b, preferred_element_type=F32, precision=precision)


def dot_nt(a, b, precision=None):
    return lax.dot_general(
        a, b, (((1,), (1,)), ((), ())), preferred_element_type=F32, precision=precision
    )


def dot_tn(a, b, precision=None):
    return lax.dot_general(
        a, b, (((0,), (0,)), ((), ())), preferred_element_type=F32, precision=precision
    )


def iota(shape, dim):
    return lax.broadcasted_iota(jnp.int32, shape, dim)


def put(ref, at, value):
    ref[0, at, :] = value[:, :128]
    ref[1, at, :] = value[:, 128:]


def got(ref, at):
    return jnp.concatenate([ref[0, at, :], ref[1, at, :]], axis=1)


THEN = {0: (4, 6, 7), 1: (5, 8, 9), 2: (10,), 3: (11,), 4: (), 5: (12, 13)}
THEN = {**THEN, 6: (14,), 7: (15,), 8: (16,), 9: (17,), 12: (18,), 13: (19,)}
PLACE = {**{m: m for m in range(10)}, 12: 21, 13: 22}
WHOLE = (0, 1, 2, 3, 6, 7, 8, 9, 12, 13)
RING = [0, 0, 1, 1, 0, 0] + [1] * 14
BACKWARD = [0, 1] * 10


def schedule(hop=1.9, rate=46600.0, later=(0.0, 7.0, 7.0, 7.0), mixer_at=14.0):
    size = {("shared", 0): 16384, ("mixed", 0): 32768}
    rank = {("shared", 0): 0.5, ("mixed", 0): 1.5}
    for c in range(CHUNKS):
        size["rows", c], size["hid", c] = 32768, 65536
        rank["rows", c] = rank["hid", c] = c
    cost = {"scan": 2.2, "pair": 0.1, "back": 0.5, "mixer": 1.9, "mix_out": 0.6, "up": 0.47, "down": 0.47}
    urgency = {"up": 1, "down": 2, "scan": 3, "pair": 3, "back": 4, "mixer": 3, "mix_out": 4}
    now, free = 0.0, [0.0] * 4
    coming, ready, events = [], [], []
    ends = {gather: [] for gather in size}
    seen = {gather: 0 for gather in size}

    def send(gather, turn, m):
        nonlocal now
        now += 0.007
        link = (RING[m] ^ turn) * 2 + BACKWARD[m]
        free[link] = max(now, free[link]) + size[gather] / (2 if m in WHOLE else 4) / rate
        if m in THEN:
            heapq.heappush(coming, (free[link] + hop, rank[gather], ("message", gather, turn, m)))
            return
        ends[gather].append(free[link] + hop)
        if len(ends[gather]) == 16:
            heapq.heappush(coming, (max(ends[gather]), rank[gather], ("leaves", gather)))

    def begin(gather):
        for m in range(4):
            for turn in (0, 1):
                send(gather, turn, m)

    for c in range(CHUNKS):
        heapq.heappush(coming, (later[c], 0.0, ("arrive", c)))
    for at, name in ((0.0, "shared"), (0.0, "scan"), (4.5, "pair"), (5.0, "back"), (mixer_at, "mixer")):
        heapq.heappush(coming, (at, 1.5, (name, 0)))
    while coming or ready:
        while coming and (coming[0][0] <= now or not ready):
            at, order, event = heapq.heappop(coming)
            now = max(now, at)
            heapq.heappush(ready, (urgency.get(event[0], 0), order, at, event))
        event = heapq.heappop(ready)[3]
        events.append(event)
        now += cost.get(event[0], 0.01)
        name, which = event[:2]
        if name in ("arrive", "shared", "mixer", "up"):
            begin(({"arrive": "rows", "up": "hid", "mixer": "mixed"}.get(name, name), which))
        if name in ("message", "leaves"):
            if name == "message":
                for m in THEN[event[3]]:
                    send(which, event[2], m)
            seen[which] += 1
            if seen[which] == 25:
                last = {"rows": "up", "hid": "down", "mixed": "mix_out"}.get(which[0])
                if last:
                    heapq.heappush(ready, (urgency[last], rank[which], now, (last, which[1])))
    return events


class Gather:
    def __init__(self, buf, send, recv, number, place):
        self.buf, self.send, self.recv, self.number = buf, send, recv, number
        self.ep, self.y, self.x = place
        self.half = buf.shape[1] // 2
        self.plan = []
        for turned in (False, True):
            messages = [(0, 0, None, 0, 1), (0, 0, None, 0, -1), (0, 0, None, 1, 1), (0, 0, None, 1, -1)]
            messages += [(-1, 0, 0, 0, 1), (1, 0, 1, 0, -1)]
            messages += [(i, 0, None, 1, d) for i in (-1, 1) for d in (1, -1)]
            messages += [(0, -1, 0, 1, 1), (0, 1, 1, 1, -1)]
            messages += [(2, 0, None, 1, 1), (2, 0, None, 1, -1)]
            messages += [(i, -d, (1 - d) // 2, 1, d) for i in (-1, 1) for d in (1, -1)]
            messages += [(2, -1, 0, 1, 1), (2, 1, 1, 1, -1)]
            self.plan += [(turned, *m) for m in messages]

    def copy(self, m):
        turned, i, j, part, ring, step = self.plan[m]
        dy, dx = (i, j) if turned else (j, i)
        shard = ((self.y + dy + 4) % 4) * 4 + (self.x + dx + 4) % 4
        start, count = (self.half if turned else 0), self.half
        if part is not None:
            count = self.half // 2
            start += part * count
        along_y = (ring == 0) == turned
        ny = (self.y + step + 4) % 4 if along_y else self.y
        nx = self.x if along_y else (self.x + step + 4) % 4
        ref = self.buf.at[shard, pl.ds(start, count)]
        stage = sum(m % 20 >= first for first in (4, 12, 18))
        arrival = PLACE.get(m % 20)
        arrival = 20 if arrival is None else arrival + (2 if arrival > 20 else 10) * (m // 20)
        return pltpu.make_async_remote_copy(
            src_ref=ref,
            dst_ref=ref,
            send_sem=self.send.at[self.number, stage],
            recv_sem=self.recv.at[self.number, arrival],
            device_id=(self.ep, ny * 4 + nx),
            device_id_type=MESH,
        )

    def whole(self, count, sem):
        ref = self.buf.at[pl.ds(0, count)]
        pltpu.make_async_copy(ref, ref, sem).wait()

    def leaves(self):
        self.whole(4, self.recv.at[self.number, 20])

    def finish(self):
        for stage, count in enumerate((4, 6, 4, 1)):
            self.whole(count, self.send.at[self.number, stage])


def factors(log_step, state):
    step_rate = jnp.exp(log_step)
    frequency = jnp.pi * state.astype(F32)
    angle = step_rate * frequency
    turn_cosine = jnp.cos(angle)
    turn_sine = jnp.sin(angle)
    base = jnp.exp(-0.5 * step_rate)
    base_real = base * turn_cosine
    starting_quadrature = base * turn_sine
    inverse = 1.0 / (0.25 + frequency * frequency)
    lowered = base_real - 1.0
    inject_real = (-0.5 * lowered + starting_quadrature * frequency) * inverse
    inject_imaginary = (-0.5 * starting_quadrature - lowered * frequency) * inverse
    return (turn_cosine, turn_sine, inject_real, inject_imaginary, -0.5 * step_rate)


def body(
    step_ref, x_hbm, shift_hbm, imap_hbm, rout_hbm, e_hbm, gain_hbm, routes_hbm, rw_hbm,
    mixw_hbm, wg_hbm, wu_hbm, wd_hbm, sg_hbm, su_hbm, sd_hbm,
    mix_ref, exp_ref,
    x_ref, shift_ref, imap_ref, rout_ref, e_ref, gain_ref, routes_ref, rw_ref, mixw, wg, wu, wd, sgu, sd,
    normed, outgoing, back_hi, back_lo, rows_buf, hid_buf, res, returned, mix_buf, sh_buf, pair, chips,
    push_r, push_i, mag, ph_r, ph_i, keep,
    load_sem, g_send, g_recv, z_send, z_recv, s_send, s_recv, r_send, r_recv,
):
    ep, tp = lax.axis_index("ep"), lax.axis_index("tp")
    z, core = ep // 2, ep % 2
    y, x = tp // 4, tp % 4

    loads = [
        pltpu.make_async_copy(src, dst, load_sem.at[k])
        for k, (src, dst) in enumerate(
            [(sg_hbm, sgu.at[0:64]), (su_hbm, sgu.at[64:128]), (wg_hbm, wg), (wu_hbm, wu),
             (wd_hbm, wd), (sd_hbm, sd), (mixw_hbm, mixw), (e_hbm, e_ref), (gain_hbm, gain_ref),
             (routes_hbm, routes_ref), (x_hbm, x_ref), (shift_hbm, shift_ref),
             (imap_hbm, imap_ref), (rout_hbm, rout_ref), (rw_hbm, rw_ref)]
        )
    ]
    for k in (7, 8, 9, 10, 11, 12, 13, 14, 0, 1, 2, 3, 4, 5, 6):
        loads[k].start()

    def far(dz, flip):
        return ((z + dz + 16) % 16) * 2 + (core + flip) % 2

    chips[...] = jnp.zeros_like(chips)
    barrier = pltpu.get_barrier_semaphore()
    for dz, flip in SLOTS[1:]:
        pl.semaphore_signal(barrier, inc=1, device_id=(far(dz, flip), tp), device_id_type=MESH)
    for ny, nx in ((y, (x + 1) % 4), (y, (x + 3) % 4), ((y + 1) % 4, x), ((y + 3) % 4, x)):
        pl.semaphore_signal(barrier, inc=1, device_id=(ep, ny * 4 + nx), device_id_type=MESH)

    with jax.named_scope("load"):
        for k in (7, 8, 9):
            loads[k].wait()
    values = e_ref[...].astype(F32)
    scale = lax.rsqrt(jnp.mean(values * values, axis=-1, keepdims=True) + 1e-06)
    normed[...] = (values * scale * gain_ref[...]).astype(BF16)
    expert = iota((32, 128), 0)
    named = [(routes_ref[k : k + 1, :] == expert).astype(F32) for k in (0, 1)]
    earlier = (iota((128, 128), 0) < iota((128, 128), 1)).astype(BF16)
    before = dot((named[0] + named[1]).astype(BF16), earlier)
    target = []
    for k in (0, 1):
        rank = jnp.sum(named[k] * before, axis=0, keepdims=True).astype(jnp.int32)
        route = routes_ref[k : k + 1, :]
        away = (z + 16 - (route >> 1)) & 15
        turn = jnp.zeros_like(route)
        for i, dz in enumerate(REACH):
            turn = jnp.where(away == dz % 16, i, turn)
        target.append((turn * 2 + ((route + core) & 1)) * CAP + rank)
    own = normed[:, pl.ds(pl.multiple_of(tp * 128, 128), 128)]

    def took(c):
        slot = iota((CHUNK, 128), 0) + c * CHUNK
        return [(target[k] == slot).astype(F32) for k in (0, 1)]

    def pack(c):
        first, second = took(c)
        outgoing[c * CHUNK : (c + 1) * CHUNK] = dot((first + second).astype(BF16), own).astype(BF16)

    pack(0)
    with jax.named_scope("enter"):
        pl.semaphore_wait(barrier, len(SLOTS) - 1 + 4)

    def send_chunk(c):
        for k in range(max(1, 8 * c), 8 * c + 8):
            dz, flip = SLOTS[k]
            pltpu.make_async_remote_copy(
                src_ref=outgoing.at[pl.ds(k * CAP, CAP)],
                dst_ref=rows_buf.at[c, tp, pl.ds((k - 8 * c) * CAP, CAP)],
                send_sem=z_send,
                recv_sem=z_recv.at[c],
                device_id=(far(-dz, flip), tp),
                device_id_type=MESH,
            ).start()

    send_chunk(0)
    rows_buf[0, tp, 0:CAP] = outgoing[0:CAP]

    def rows_arrived(c):
        if c == 0:
            ref = rows_buf.at[0, tp, pl.ds(CAP, CHUNK - CAP)]
        else:
            ref = rows_buf.at[c, tp]
        pltpu.make_async_copy(ref, ref, z_recv.at[c]).wait()

    def to_partner():
        return pltpu.make_async_remote_copy(
            src_ref=pair.at[core],
            dst_ref=pair.at[core],
            send_sem=s_send.at[0],
            recv_sem=s_recv.at[0],
            device_id=(far(0, 1), tp),
            device_id_type=MESH,
        )

    def to_chip(dz):
        return pltpu.make_async_remote_copy(
            src_ref=chips.at[z],
            dst_ref=chips.at[z],
            send_sem=s_send.at[dz],
            recv_sem=s_recv.at[dz],
            device_id=(far(dz, 0), tp),
            device_id_type=MESH,
        )

    def parts_of(ref, i):
        return [ref[i, 2 * n : 2 * n + 2, :] for n in range(4)]

    def after(early_r, early_i, late):
        a_r, a_i, c_r, c_i = late
        return a_r * early_r - a_i * early_i + c_r, a_r * early_i + a_i * early_r + c_i

    def pair_part():
        to_partner().wait_recv()
        first, second = parts_of(pair, 0), parts_of(pair, 1)
        a_r, a_i = first[0] * second[0] - first[1] * second[1], first[0] * second[1] + first[1] * second[0]
        c_r, c_i = after(first[2], first[3], second)
        for n, part in enumerate((a_r, a_i, c_r, c_i)):
            chips[z, 2 * n : 2 * n + 2, :] = part
        for dz in range(1, 16):

            @pl.when(z + dz < 16)
            def _(dz=dz):
                to_chip(dz).start()

    def scan_part():
        with jax.named_scope("load2"):
            for k in (10, 11, 12):
                loads[k].wait()
        group = iota((1, 256), 1) // 64
        log_step = jnp.where(group == 0, step_ref[0], step_ref[1])
        log_step = jnp.where(group == 2, step_ref[2], log_step)
        log_step = jnp.where(group == 3, step_ref[3], log_step)
        cosine, sine, inj_r, inj_i, low = factors(log_step, iota((1, 256), 1) % 64)
        spread = (iota((64, 256), 1) % 64 == iota((64, 256), 0)).astype(BF16)
        mine = iota((64, 256), 0) // 16 == iota((64, 256), 1) // 64
        drive_r, drive_i = [
            dot_tn(
                x_ref[...],
                jnp.where(mine, dot(imap_ref[64 * c : 64 * c + 64, :], spread), 0.0).astype(BF16),
            )
            for c in (0, 1)
        ]
        every = slice(None)
        put(push_r, every, inj_r * drive_r - inj_i * drive_i)
        put(push_i, every, inj_r * drive_i + inj_i * drive_r)
        of_group = (iota((4, 256), 1) // 64 == iota((4, 256), 0)).astype(F32)
        put(mag, every, jnp.exp(low + dot_tn(shift_ref[...], of_group, HIGHEST)))
        state_r, state_i = jnp.zeros((8, 256), F32), jnp.zeros((8, 256), F32)
        total = jnp.ones((8, 256), F32)
        turn_r, turn_i = jnp.ones((1, 256), F32), jnp.zeros((1, 256), F32)
        for j in range(32):
            at = pl.ds(j, 8, stride=32)
            m = got(mag, at)
            d_r, d_i = m * cosine, m * sine
            state_r, state_i = (
                d_r * state_r - d_i * state_i + got(push_r, at),
                d_r * state_i + d_i * state_r + got(push_i, at),
            )
            total = total * m
            turn_r, turn_i = turn_r * cosine - turn_i * sine, turn_r * sine + turn_i * cosine
            put(push_r, at, state_r)
            put(push_i, at, state_i)
            put(mag, at, total)
            ph_r[j : j + 1, :] = turn_r
            ph_i[j : j + 1, :] = turn_i
        all_r, all_i = total * turn_r, total * turn_i
        c_r, c_i = jnp.zeros((1, 256), F32), jnp.zeros((1, 256), F32)
        t_r, t_i = jnp.ones((1, 256), F32), jnp.zeros((1, 256), F32)
        for s in range(8):
            for n, part in enumerate((t_r, t_i, c_r, c_i)):
                keep[n, s : s + 1, :] = part
            a_r, a_i = all_r[s : s + 1], all_i[s : s + 1]
            c_r, c_i = (
                a_r * c_r - a_i * c_i + state_r[s : s + 1],
                a_r * c_i + a_i * c_r + state_i[s : s + 1],
            )
            t_r, t_i = a_r * t_r - a_i * t_i, a_r * t_i + a_i * t_r
        for n, part in enumerate((t_r, t_i, c_r, c_i)):
            pair[core, 2 * n : 2 * n + 1, :] = part[:, :128]
            pair[core, 2 * n + 1 : 2 * n + 2, :] = part[:, 128:]
        to_partner().start()

    place = (ep, y, x)
    rows = [Gather(rows_buf.at[c], g_send, g_recv, c, place) for c in range(CHUNKS)]
    hid = [Gather(hid_buf.at[c], g_send, g_recv, CHUNKS + c, place) for c in range(CHUNKS)]
    mixed = Gather(mix_buf, g_send, g_recv, 2 * CHUNKS, place)
    shared = Gather(sh_buf, g_send, g_recv, 2 * CHUNKS + 1, place)

    def packed(top, bottom):
        first = (iota((64, 128), 1) == iota((64, 128), 0)).astype(BF16)
        second = (iota((64, 128), 1) == iota((64, 128), 0) + 64).astype(BF16)
        return (dot(top, first) + dot(bottom, second)).astype(BF16)

    def silu(v):
        return v / (1.0 + jnp.exp(-v))

    def shared_part():
        loads[0].wait()
        loads[1].wait()
        both_sums = dot_nt(normed[...], sgu[...])
        hidden = (silu(both_sums[:, :64]) * both_sums[:, 64:]).astype(BF16)
        sh_buf[tp] = packed(hidden[:64], hidden[64:])

    def mixer_part():
        with jax.named_scope("sums"):
            for dz in range(1, 16):

                @pl.when(z - dz >= 0)
                def _(dz=dz):
                    to_chip(dz).wait_recv()

        in_r, in_i = jnp.zeros((2, 128), F32), jnp.zeros((2, 128), F32)
        for i in range(15):
            n_r, n_i = after(in_r, in_i, parts_of(chips, i))
            in_r, in_i = jnp.where(i < z, n_r, in_r), jnp.where(i < z, n_i, in_i)
        n_r, n_i = after(in_r, in_i, parts_of(pair, 0))
        in_r, in_i = jnp.where(core == 1, n_r, in_r), jnp.where(core == 1, n_i, in_i)
        in_r = jnp.concatenate([in_r[0:1], in_r[1:2]], axis=1)
        in_i = jnp.concatenate([in_i[0:1], in_i[1:2]], axis=1)
        k_r, k_i = keep[0], keep[1]
        car_r = k_r * in_r - k_i * in_i + keep[2]
        car_i = k_r * in_i + k_i * in_r + keep[3]
        for j in range(32):
            at = pl.ds(j, 8, stride=32)
            p_r, p_i, m = ph_r[j : j + 1, :], ph_i[j : j + 1, :], got(mag, at)
            put(push_r, at, got(push_r, at) + m * (p_r * car_r - p_i * car_i))
            put(push_i, at, got(push_i, at) + m * (p_r * car_i + p_i * car_r))
        loads[13].wait()
        spread = (iota((64, 256), 1) % 64 == iota((64, 256), 0)).astype(F32)
        mine = iota((64, 256), 0) // 16 == iota((64, 256), 1) // 64
        out_r = jnp.where(mine, dot(rout_ref[0:64, :], spread, HIGHEST), 0.0)
        out_i = jnp.where(mine, dot(rout_ref[64:128, :], spread, HIGHEST), 0.0)
        every = slice(None)
        v = dot_nt(got(push_r, every), out_r, HIGHEST) - dot_nt(got(push_i, every), out_i, HIGHEST)
        act = 0.5 * v * (1.0 + jnp.tanh(0.7978845608 * (v + 0.044715 * v * v * v)))
        act = act.astype(BF16)
        mix_buf[tp] = packed(act[:128], act[128:])

    def joined(ref):
        return jnp.concatenate([ref[s] for s in range(16)], axis=1)

    def up_part(c):
        if c == 0:
            loads[2].wait()
            loads[3].wait()
        piece = joined(rows_buf.at[c])
        hid_buf[c, tp] = (silu(dot(piece, wg[...])) * dot(piece, wu[...])).astype(BF16)

    def down_part(c):
        if c == 0:
            loads[4].wait()
        res[c * CHUNK : (c + 1) * CHUNK] = dot(joined(hid_buf.at[c]), wd[...]).astype(BF16)
        for k in range(8 * c, 8 * c + 8):
            if k == 0:
                returned[0:CAP] = res[0:CAP]
                continue
            pltpu.make_async_remote_copy(
                src_ref=res.at[pl.ds(k * CAP, CAP)],
                dst_ref=returned.at[pl.ds(k * CAP, CAP)],
                send_sem=r_send,
                recv_sem=r_recv.at[c],
                device_id=(far(*SLOTS[k]), tp),
                device_id_type=MESH,
            ).start()

    def spread_out(buf, weight):
        height = buf.shape[1]
        low_half = iota((height, 128), 1) < 64
        total = jnp.zeros((2 * height, 128), F32)
        for s in range(16):
            block = buf[s]
            zero = jnp.zeros_like(block)
            both_rows = jnp.concatenate(
                [jnp.where(low_half, block, zero), jnp.where(low_half, zero, block)], axis=0
            )
            w = weight[s * 64 : (s + 1) * 64]
            total += dot(both_rows, jnp.concatenate([w, w], axis=0))
        return total

    def back_part():
        loads[14].wait()
        for c in range(CHUNKS):
            first, second = took(c)
            weighted = jnp.transpose(first * rw_ref[0:1, :] + second * rw_ref[1:2, :])
            rounded = weighted.astype(BF16)
            columns = slice(c * CHUNK, (c + 1) * CHUNK)
            back_hi[:, columns] = rounded
            back_lo[:, columns] = (weighted - rounded.astype(F32)).astype(BF16)

    def gain_part(c):
        with jax.named_scope(f"back{c}"):
            some = slice(CAP if c == 0 else c * CHUNK, (c + 1) * CHUNK)
            came = returned.at[some]
            pltpu.make_async_copy(came, came, r_recv.at[c]).wait()
        some = slice(c * CHUNK, (c + 1) * CHUNK)
        block = returned[some]
        return dot(back_hi[:, some], block) + dot(back_lo[:, some], block)

    gathers = {("shared", 0): shared, ("mixed", 0): mixed}
    for c in range(CHUNKS):
        gathers["rows", c], gathers["hid", c] = rows[c], hid[c]

    def begin(gather):
        for m in range(4):
            for turn in (0, 20):
                gather.copy(turn + m).start()

    shared_part()
    for event in schedule():
        name, which = event[:2]
        if name == "message":
            _, gather, turn, m = event
            gathers[gather].copy(20 * turn + m).wait_recv()
            for following in THEN[m]:
                gathers[gather].copy(20 * turn + following).start()
        elif name == "leaves":
            gathers[which].leaves()
        elif name == "arrive":
            with jax.named_scope(f"arrive{which}"):
                rows_arrived(which)
            begin(rows[which])
            if which == 0:
                for c in (1, 2, 3):
                    pack(c)
                    send_chunk(c)
        elif name == "shared":
            begin(shared)
        elif name == "scan":
            with jax.named_scope("scan"):
                scan_part()
        elif name == "pair":
            pair_part()
        elif name == "back":
            with jax.named_scope("back"):
                back_part()
        elif name == "mixer":
            with jax.named_scope("mixer_part"):
                mixer_part()
            begin(mixed)
        elif name == "up":
            with jax.named_scope(f"up{which}"):
                up_part(which)
            begin(hid[which])
        elif name == "down":
            with jax.named_scope(f"down{which}"):
                down_part(which)
        elif name == "mix_out":
            with jax.named_scope("mix_out"):
                loads[6].wait()
                mix_ref[...] = spread_out(mix_buf, mixw).astype(BF16)
    loads[5].wait()
    common = spread_out(sh_buf, sd)
    for c in range(CHUNKS - 1):
        common += gain_part(c)

    with jax.named_scope("finish"):
        for gather in rows + hid + [mixed, shared]:
            gather.finish()
        to_partner().wait_send()
        for dz in range(1, 16):

            @pl.when(z + dz < 16)
            def _(dz=dz):
                to_chip(dz).wait_send()

    sent = outgoing.at[pl.ds(0, 31 * CAP)]
    pltpu.make_async_copy(sent, sent, z_send).wait()
    back = returned.at[pl.ds(0, 31 * CAP)]
    pltpu.make_async_copy(back, back, r_send).wait()
    common += gain_part(CHUNKS - 1)
    exp_ref[...] = common.astype(BF16)


def shards(
    mixer_input, log_step, decay_shift, input_map, readout, mixer_weight, expert_input,
    norm_gain, routes, route_weight, expert_switch_matrix, up_weight, down_weight,
    shared_gate, shared_up, shared_down,
):
    vmem = pl.BlockSpec(memory_space=pltpu.VMEM)
    hbm = pl.BlockSpec(memory_space=pltpu.HBM)
    V, DMA = pltpu.VMEM, pltpu.SemaphoreType.DMA
    return pl.pallas_call(
        body,
        out_shape=(
            jax.ShapeDtypeStruct((256, 128), BF16),
            jax.ShapeDtypeStruct((128, 128), BF16),
        ),
        in_specs=[pl.BlockSpec(memory_space=pltpu.SMEM)] + [hbm] * 15,
        out_specs=(vmem, vmem),
        scratch_shapes=[
            V((64, 256), BF16),
            V((4, 256), F32),
            V((128, 64), BF16),
            V((128, 64), F32),
            V((128, 2048), BF16),
            V((1, 2048), F32),
            V((2, 128), jnp.int32),
            V((2, 128), F32),
            V((1024, 128), BF16),
            V((2048, 256), BF16),
            V((2048, 256), BF16),
            V((4096, 128), BF16),
            V((128, 2048), BF16),
            V((1024, 128), BF16),
            V((128, 2048), BF16),
            V((512, 128), BF16),
            V((128, 512), BF16),
            V((128, 512), BF16),
            V((CHUNKS, 16, CHUNK, 128), BF16),
            V((CHUNKS, 16, CHUNK, 256), BF16),
            V((512, 128), BF16),
            V((512, 128), BF16),
            V((16, 128, 128), BF16),
            V((16, 64, 128), BF16),
            V((2, 8, 128), F32),
            V((16, 8, 128), F32),
            V((2, 256, 128), F32),
            V((2, 256, 128), F32),
            V((2, 256, 128), F32),
            V((32, 256), F32),
            V((32, 256), F32),
            V((4, 8, 256), F32),
            DMA((15,)),
            DMA((2 * CHUNKS + 2, 4)),
            DMA((2 * CHUNKS + 2, 25)),
            DMA,
            DMA((CHUNKS,)),
            DMA((16,)),
            DMA((16,)),
            DMA,
            DMA((CHUNKS,)),
        ],
        compiler_params=pltpu.CompilerParams(
            collective_id=0, has_side_effects=True, vmem_limit_bytes=67_043_328
        ),
    )(
        log_step,
        mixer_input.T,
        decay_shift.T,
        jnp.swapaxes(input_map, 2, 3).reshape(128, 64),
        readout.reshape(128, 64),
        expert_input,
        norm_gain.reshape(1, 2048),
        routes.T,
        route_weight.T,
        mixer_weight,
        expert_switch_matrix[0],
        up_weight[0],
        down_weight[0],
        shared_gate.T,
        shared_up.T,
        shared_down,
    )


def solution(mesh):
    placed = (
        P("ep", "tp"),
        P("tp"),
        P("ep", "tp"),
        P(None, "tp", None, None),
        P(None, "tp", None, None),
        P(None, "tp"),
        P("ep", None),
        P(),
        P("ep", None),
        P("ep", None),
        P("ep", None, "tp"),
        P("ep", None, "tp"),
        P("ep", None, "tp"),
        P(None, "tp"),
        P(None, "tp"),
        P(None, "tp"),
    )
    return jax.shard_map(
        shards, mesh=mesh, in_specs=placed, out_specs=(P("ep", "tp"), P("ep", "tp")), check_vma=False
    )
```

```python
import heapq

import jax
import jax.numpy as jnp
from jax import lax
from jax.experimental import pallas as pl
from jax.experimental.pallas import tpu as pltpu
from jax.sharding import PartitionSpec as P

MESH = pl.DeviceIdType.MESH
F32 = jnp.float32
BF16 = jnp.bfloat16
HIGHEST = lax.Precision.HIGHEST

CHUNKS = 4
CHUNK = 128
CAP = 16
REACH = [0, 1, -1, 2, -4, 5, -5, 6, -6, 7, -7, 8, -2, 3, -3, 4]
SLOTS = [(dz, flip) for dz in REACH for flip in (0, 1)]


def dot(a, b, precision=None):
    return jnp.dot(a, b, preferred_element_type=F32, precision=precision)


def dot_nt(a, b, precision=None):
    return lax.dot_general(
        a, b, (((1,), (1,)), ((), ())), preferred_element_type=F32, precision=precision
    )


def dot_tn(a, b, precision=None):
    return lax.dot_general(
        a, b, (((0,), (0,)), ((), ())), preferred_element_type=F32, precision=precision
    )


def iota(shape, dim):
    return lax.broadcasted_iota(jnp.int32, shape, dim)


def put(ref, at, value):
    ref[0, at, :] = value[:, :128]
    ref[1, at, :] = value[:, 128:]


def got(ref, at):
    return jnp.concatenate([ref[0, at, :], ref[1, at, :]], axis=1)


THEN = {0: (4, 6, 7), 1: (5, 8, 9), 2: (10,), 3: (11,), 4: (12, 13), 5: (12, 13)}
THEN = {**THEN, 6: (14,), 7: (15,), 8: (16,), 9: (17,), 12: (18,), 13: (19,)}
PLACE = {**{m: m for m in range(10)}, 12: 21, 13: 22}
WHOLE = (0, 1, 2, 3, 6, 7, 8, 9, 12, 13)
RING = [0, 0, 1, 1, 0, 0] + [1] * 14
BACKWARD = [0, 1] * 10


def passed_on(here, gather, turn, m):
    here.add((gather, turn, m))
    if m in (4, 5) and (gather, turn, 9 - m) not in here:
        return ()
    return THEN[m]


def schedule(hop=2.3, rate=43000.0, later=(0.0, 7.0, 7.0, 14.0), mixer_at=28.0, trace=None):
    size = {("shared", 0): 16384, ("mixed", 0): 32768}
    rank = {("shared", 0): 0.5, ("mixed", 0): 3.5}
    for c in range(CHUNKS):
        size["rows", c] = 32768
        rank["rows", c] = c
    cost = {"scan": 2.2, "pair": 0.1, "back": 0.3, "mixer": 1.9, "mix_out": 0.6, "up": 0.47, "down": 0.35, "sum": 0.1}
    urgency = {"up": 1, "down": 1, "scan": 3, "pair": 3, "back": 4, "mixer": 3, "mix_out": 4, "sum": 0}
    now, free = 0.0, [0.5] * 4
    coming, ready, events = [], [], []
    ends = {gather: [] for gather in size}
    seen = {gather: 0 for gather in size}
    count, here = {}, set()

    def use(link, amount):
        nonlocal now
        now += 0.007
        free[link] = max(now, free[link]) + amount / rate
        return free[link] + hop

    def later_on(at, order, event):
        heapq.heappush(coming, (at, order, event))

    def send(gather, turn, m):
        link = (RING[m] ^ turn) * 2 + BACKWARD[m]
        at = use(link, size[gather] / (2 if m in WHOLE else 4))
        if m in THEN:
            later_on(at, rank[gather], ("message", gather, turn, m))
            return
        ends[gather].append(at)
        if len(ends[gather]) == 16:
            later_on(max(ends[gather]), rank[gather], ("leaves", gather))

    def begin(gather):
        for m in range(4):
            for turn in (0, 1):
                send(gather, turn, m)

    for c in range(CHUNKS):
        later_on(later[c], 0.0, ("arrive", c))
    for at, name in ((0.0, "shared"), (0.0, "scan"), (4.5, "pair"), (5.0, "back"), (mixer_at, "mixer")):
        later_on(at, 1.5, (name, 0))
    for at, event in ((0.02, ("relay", 0)), (1.0, ("relay", 1)), (1.5, ("weights", 2)), (4.5, ("weights", 3))):
        later_on(at, 9.0, event)
    while coming or ready:
        while coming and (coming[0][0] <= now or not ready):
            at, order, event = heapq.heappop(coming)
            now = max(now, at)
            heapq.heappush(ready, (urgency.get(event[0], 0), order, at, event))
        event = heapq.heappop(ready)[3]
        events.append(event)
        if trace is not None:
            trace[event] = now
        now += cost.get(event[0], 0.01)
        name, which = event[:2]
        if name in ("arrive", "shared", "mixer"):
            begin(({"arrive": "rows", "mixer": "mixed"}.get(name, name), which))
        elif name == "weights":
            for link in range(4):
                use(link, 65536)
            later_on(max(use(link, 32768) for link in range(4)), 9.0, ("relay", which))
        elif name == "relay":
            for link in range(4):
                use(link, 32768)
        elif name == "up":
            for turn in (0, 1):
                for side in (0, 1):
                    later_on(use(2 * turn + side, 32768), which, ("near", which, turn, side))
        elif name == "near":
            turn, side = event[2:]
            at = use(2 * turn + side, 16384)
            count.setdefault((which, turn), []).append(at)
            if len(count[which, turn]) == 2:
                later_on(max(count[which, turn]), which, ("down", which, turn))
        elif name == "down":
            turn = 1 - event[2]
            at = max(use(2 * turn + side, 16384) for side in (0, 0, 1))
            count.setdefault(which, []).append(at)
            if len(count[which]) == 2:
                later_on(max(count[which]) + 0.5, which, ("sum", which))
        elif name in ("message", "leaves"):
            if name == "message":
                for m in passed_on(here, which, *event[2:]):
                    send(which, event[2], m)
            seen[which] += 1
            if seen[which] == 25:
                last = {"rows": "up", "mixed": "mix_out"}.get(which[0])
                if last:
                    heapq.heappush(ready, (urgency[last], rank[which], now, (last, which[1])))
    return events


class Gather:
    def __init__(self, buf, send, recv, number, place):
        self.buf, self.send, self.recv, self.number = buf, send, recv, number
        self.ep, self.y, self.x = place
        self.half = buf.shape[1] // 2
        self.plan = []
        for turned in (False, True):
            messages = [(0, 0, None, 0, 1), (0, 0, None, 0, -1), (0, 0, None, 1, 1), (0, 0, None, 1, -1)]
            messages += [(-1, 0, 0, 0, 1), (1, 0, 1, 0, -1)]
            messages += [(i, 0, None, 1, d) for i in (-1, 1) for d in (1, -1)]
            messages += [(0, -1, 0, 1, 1), (0, 1, 1, 1, -1)]
            messages += [(2, 0, None, 1, 1), (2, 0, None, 1, -1)]
            messages += [(i, -d, (1 - d) // 2, 1, d) for i in (-1, 1) for d in (1, -1)]
            messages += [(2, -1, 0, 1, 1), (2, 1, 1, 1, -1)]
            self.plan += [(turned, *m) for m in messages]

    def copy(self, m):
        turned, i, j, part, ring, step = self.plan[m]
        dy, dx = (i, j) if turned else (j, i)
        shard = ((self.y + dy + 4) % 4) * 4 + (self.x + dx + 4) % 4
        start, count = (self.half if turned else 0), self.half
        if part is not None:
            count = self.half // 2
            start += part * count
        along_y = (ring == 0) == turned
        ny = (self.y + step + 4) % 4 if along_y else self.y
        nx = self.x if along_y else (self.x + step + 4) % 4
        ref = self.buf.at[shard, pl.ds(start, count)]
        stage = sum(m % 20 >= first for first in (4, 12, 18))
        arrival = PLACE.get(m % 20)
        arrival = 20 if arrival is None else arrival + (2 if arrival > 20 else 10) * (m // 20)
        return pltpu.make_async_remote_copy(
            src_ref=ref,
            dst_ref=ref,
            send_sem=self.send.at[self.number, stage],
            recv_sem=self.recv.at[self.number, arrival],
            device_id=(self.ep, ny * 4 + nx),
            device_id_type=MESH,
        )

    def whole(self, count, sem):
        ref = self.buf.at[pl.ds(0, count)]
        pltpu.make_async_copy(ref, ref, sem).wait()

    def leaves(self):
        self.whole(4, self.recv.at[self.number, 20])

    def finish(self):
        for stage, count in enumerate((4, 6, 4, 1)):
            self.whole(count, self.send.at[self.number, stage])


def factors(log_step, state):
    step_rate = jnp.exp(log_step)
    frequency = jnp.pi * state.astype(F32)
    angle = step_rate * frequency
    turn_cosine = jnp.cos(angle)
    turn_sine = jnp.sin(angle)
    base = jnp.exp(-0.5 * step_rate)
    base_real = base * turn_cosine
    starting_quadrature = base * turn_sine
    inverse = 1.0 / (0.25 + frequency * frequency)
    lowered = base_real - 1.0
    inject_real = (-0.5 * lowered + starting_quadrature * frequency) * inverse
    inject_imaginary = (-0.5 * starting_quadrature - lowered * frequency) * inverse
    return (turn_cosine, turn_sine, inject_real, inject_imaginary, -0.5 * step_rate)


def body(
    step_ref, x_hbm, shift_hbm, imap_hbm, rout_hbm, e_hbm, gain_hbm, routes_hbm, rw_hbm,
    mixw_hbm, wg_hbm, wu_hbm, wd_hbm, sg_hbm, su_hbm, sd_hbm,
    mix_ref, exp_ref,
    x_ref, shift_ref, imap_ref, rout_ref, e_ref, gain_ref, routes_ref, rw_ref, mixw, wg, wu, wd, wd_of, relay, sgu, sd,
    normed, outgoing, back_hi, back_lo, rows_buf, hid_buf, part, parts, res, returned, mix_buf, sh_buf, pair, chips,
    push_r, push_i, mag, ph_r, ph_i, keep,
    load_sem, g_send, g_recv, h_send, h_recv, w_send, w_recv, relay_recv, z_send, z_recv, s_send, s_recv, r_send, r_recv,
):
    ep, tp = lax.axis_index("ep"), lax.axis_index("tp")
    z, core = ep // 2, ep % 2
    y, x = tp // 4, tp % 4

    loads = [
        pltpu.make_async_copy(src, dst, load_sem.at[k])
        for k, (src, dst) in enumerate(
            [(sg_hbm, sgu.at[0:64]), (su_hbm, sgu.at[64:128]), (wg_hbm, wg), (wu_hbm, wu),
             (wd_hbm, wd), (sd_hbm, sd), (mixw_hbm, mixw), (e_hbm, e_ref), (gain_hbm, gain_ref),
             (routes_hbm, routes_ref), (x_hbm, x_ref), (shift_hbm, shift_ref),
             (imap_hbm, imap_ref), (rout_hbm, rout_ref), (rw_hbm, rw_ref)]
        )
    ]
    for k in (7, 8, 9, 10, 11, 12, 13, 14, 0, 1, 2, 3, 4, 5, 6):
        loads[k].start()

    def far(dz, flip):
        return ((z + dz + 16) % 16) * 2 + (core + flip) % 2

    chips[...] = jnp.zeros_like(chips)
    barrier = pltpu.get_barrier_semaphore()
    for dz, flip in SLOTS[1:]:
        pl.semaphore_signal(barrier, inc=1, device_id=(far(dz, flip), tp), device_id_type=MESH)
    for ny, nx in [(y, (x + d) % 4) for d in (1, 2, 3)] + [((y + d) % 4, x) for d in (1, 2, 3)]:
        pl.semaphore_signal(barrier, inc=1, device_id=(ep, ny * 4 + nx), device_id_type=MESH)

    with jax.named_scope("load"):
        for k in (7, 8, 9):
            loads[k].wait()
    values = e_ref[...].astype(F32)
    scale = lax.rsqrt(jnp.mean(values * values, axis=-1, keepdims=True) + 1e-06)
    normed[...] = (values * scale * gain_ref[...]).astype(BF16)
    expert = iota((32, 128), 0)
    named = [(routes_ref[k : k + 1, :] == expert).astype(F32) for k in (0, 1)]
    earlier = (iota((128, 128), 0) < iota((128, 128), 1)).astype(BF16)
    before = dot((named[0] + named[1]).astype(BF16), earlier)
    target = []
    for k in (0, 1):
        rank = jnp.sum(named[k] * before, axis=0, keepdims=True).astype(jnp.int32)
        route = routes_ref[k : k + 1, :]
        away = (z + 16 - (route >> 1)) & 15
        turn = jnp.zeros_like(route)
        for i, dz in enumerate(REACH):
            turn = jnp.where(away == dz % 16, i, turn)
        target.append((turn * 2 + ((route + core) & 1)) * CAP + rank)
    own = normed[:, pl.ds(pl.multiple_of(tp * 128, 128), 128)]

    def took(c):
        slot = iota((CHUNK, 128), 0) + c * CHUNK
        return [(target[k] == slot).astype(F32) for k in (0, 1)]

    def pack(c):
        first, second = took(c)
        outgoing[c * CHUNK : (c + 1) * CHUNK] = dot((first + second).astype(BF16), own).astype(BF16)

    pack(0)
    with jax.named_scope("enter"):
        pl.semaphore_wait(barrier, len(SLOTS) - 1 + 6)

    def send_chunk(c):
        for k in range(max(1, 8 * c), 8 * c + 8):
            dz, flip = SLOTS[k]
            pltpu.make_async_remote_copy(
                src_ref=outgoing.at[pl.ds(k * CAP, CAP)],
                dst_ref=rows_buf.at[c, tp, pl.ds((k - 8 * c) * CAP, CAP)],
                send_sem=z_send,
                recv_sem=z_recv.at[c],
                device_id=(far(-dz, flip), tp),
                device_id_type=MESH,
            ).start()

    send_chunk(0)
    rows_buf[0, tp, 0:CAP] = outgoing[0:CAP]

    def rows_arrived(c):
        if c == 0:
            ref = rows_buf.at[0, tp, pl.ds(CAP, CHUNK - CAP)]
        else:
            ref = rows_buf.at[c, tp]
        pltpu.make_async_copy(ref, ref, z_recv.at[c]).wait()

    def to_partner():
        return pltpu.make_async_remote_copy(
            src_ref=pair.at[core],
            dst_ref=pair.at[core],
            send_sem=s_send.at[0],
            recv_sem=s_recv.at[0],
            device_id=(far(0, 1), tp),
            device_id_type=MESH,
        )

    def to_chip(dz):
        return pltpu.make_async_remote_copy(
            src_ref=chips.at[z],
            dst_ref=chips.at[z],
            send_sem=s_send.at[dz],
            recv_sem=s_recv.at[dz],
            device_id=(far(dz, 0), tp),
            device_id_type=MESH,
        )

    def parts_of(ref, i):
        return [ref[i, 2 * n : 2 * n + 2, :] for n in range(4)]

    def after(early_r, early_i, late):
        a_r, a_i, c_r, c_i = late
        return a_r * early_r - a_i * early_i + c_r, a_r * early_i + a_i * early_r + c_i

    def pair_part():
        to_partner().wait_recv()
        first, second = parts_of(pair, 0), parts_of(pair, 1)
        a_r, a_i = first[0] * second[0] - first[1] * second[1], first[0] * second[1] + first[1] * second[0]
        c_r, c_i = after(first[2], first[3], second)
        for n, part in enumerate((a_r, a_i, c_r, c_i)):
            chips[z, 2 * n : 2 * n + 2, :] = part
        for dz in range(1, 16):

            @pl.when(z + dz < 16)
            def _(dz=dz):
                to_chip(dz).start()

    def scan_part():
        with jax.named_scope("load2"):
            for k in (10, 11, 12):
                loads[k].wait()
        group = iota((1, 256), 1) // 64
        log_step = jnp.where(group == 0, step_ref[0], step_ref[1])
        log_step = jnp.where(group == 2, step_ref[2], log_step)
        log_step = jnp.where(group == 3, step_ref[3], log_step)
        cosine, sine, inj_r, inj_i, low = factors(log_step, iota((1, 256), 1) % 64)
        spread = (iota((64, 256), 1) % 64 == iota((64, 256), 0)).astype(BF16)
        mine = iota((64, 256), 0) // 16 == iota((64, 256), 1) // 64
        drive_r, drive_i = [
            dot_tn(
                x_ref[...],
                jnp.where(mine, dot(imap_ref[64 * c : 64 * c + 64, :], spread), 0.0).astype(BF16),
            )
            for c in (0, 1)
        ]
        every = slice(None)
        put(push_r, every, inj_r * drive_r - inj_i * drive_i)
        put(push_i, every, inj_r * drive_i + inj_i * drive_r)
        of_group = (iota((4, 256), 1) // 64 == iota((4, 256), 0)).astype(F32)
        put(mag, every, jnp.exp(low + dot_tn(shift_ref[...], of_group, HIGHEST)))
        state_r, state_i = jnp.zeros((8, 256), F32), jnp.zeros((8, 256), F32)
        total = jnp.ones((8, 256), F32)
        turn_r, turn_i = jnp.ones((1, 256), F32), jnp.zeros((1, 256), F32)
        for j in range(32):
            at = pl.ds(j, 8, stride=32)
            m = got(mag, at)
            d_r, d_i = m * cosine, m * sine
            state_r, state_i = (
                d_r * state_r - d_i * state_i + got(push_r, at),
                d_r * state_i + d_i * state_r + got(push_i, at),
            )
            total = total * m
            turn_r, turn_i = turn_r * cosine - turn_i * sine, turn_r * sine + turn_i * cosine
            put(push_r, at, state_r)
            put(push_i, at, state_i)
            put(mag, at, total)
            ph_r[j : j + 1, :] = turn_r
            ph_i[j : j + 1, :] = turn_i
        all_r, all_i = total * turn_r, total * turn_i
        c_r, c_i = jnp.zeros((1, 256), F32), jnp.zeros((1, 256), F32)
        t_r, t_i = jnp.ones((1, 256), F32), jnp.zeros((1, 256), F32)
        for s in range(8):
            for n, part in enumerate((t_r, t_i, c_r, c_i)):
                keep[n, s : s + 1, :] = part
            a_r, a_i = all_r[s : s + 1], all_i[s : s + 1]
            c_r, c_i = (
                a_r * c_r - a_i * c_i + state_r[s : s + 1],
                a_r * c_i + a_i * c_r + state_i[s : s + 1],
            )
            t_r, t_i = a_r * t_r - a_i * t_i, a_r * t_i + a_i * t_r
        for n, part in enumerate((t_r, t_i, c_r, c_i)):
            pair[core, 2 * n : 2 * n + 1, :] = part[:, :128]
            pair[core, 2 * n + 1 : 2 * n + 2, :] = part[:, 128:]
        to_partner().start()

    place = (ep, y, x)
    rows = [Gather(rows_buf.at[c], g_send, g_recv, c, place) for c in range(CHUNKS)]
    mixed = Gather(mix_buf, g_send, g_recv, CHUNKS, place)
    shared = Gather(sh_buf, g_send, g_recv, CHUNKS + 1, place)

    def packed(top, bottom):
        first = (iota((64, 128), 1) == iota((64, 128), 0)).astype(BF16)
        second = (iota((64, 128), 1) == iota((64, 128), 0) + 64).astype(BF16)
        return (dot(top, first) + dot(bottom, second)).astype(BF16)

    def silu(v):
        return v / (1.0 + jnp.exp(-v))

    def shared_part():
        loads[0].wait()
        loads[1].wait()
        both_sums = dot_nt(normed[...], sgu[...])
        hidden = (silu(both_sums[:, :64]) * both_sums[:, 64:]).astype(BF16)
        sh_buf[tp] = packed(hidden[:64], hidden[64:])

    def mixer_part():
        with jax.named_scope("sums"):
            for dz in range(1, 16):

                @pl.when(z - dz >= 0)
                def _(dz=dz):
                    to_chip(dz).wait_recv()

        in_r, in_i = jnp.zeros((2, 128), F32), jnp.zeros((2, 128), F32)
        for i in range(15):
            n_r, n_i = after(in_r, in_i, parts_of(chips, i))
            in_r, in_i = jnp.where(i < z, n_r, in_r), jnp.where(i < z, n_i, in_i)
        n_r, n_i = after(in_r, in_i, parts_of(pair, 0))
        in_r, in_i = jnp.where(core == 1, n_r, in_r), jnp.where(core == 1, n_i, in_i)
        in_r = jnp.concatenate([in_r[0:1], in_r[1:2]], axis=1)
        in_i = jnp.concatenate([in_i[0:1], in_i[1:2]], axis=1)
        k_r, k_i = keep[0], keep[1]
        car_r = k_r * in_r - k_i * in_i + keep[2]
        car_i = k_r * in_i + k_i * in_r + keep[3]
        for j in range(32):
            at = pl.ds(j, 8, stride=32)
            p_r, p_i, m = ph_r[j : j + 1, :], ph_i[j : j + 1, :], got(mag, at)
            put(push_r, at, got(push_r, at) + m * (p_r * car_r - p_i * car_i))
            put(push_i, at, got(push_i, at) + m * (p_r * car_i + p_i * car_r))
        loads[13].wait()
        spread = (iota((64, 256), 1) % 64 == iota((64, 256), 0)).astype(F32)
        mine = iota((64, 256), 0) // 16 == iota((64, 256), 1) // 64
        out_r = jnp.where(mine, dot(rout_ref[0:64, :], spread, HIGHEST), 0.0)
        out_i = jnp.where(mine, dot(rout_ref[64:128, :], spread, HIGHEST), 0.0)
        every = slice(None)
        v = dot_nt(got(push_r, every), out_r, HIGHEST) - dot_nt(got(push_i, every), out_i, HIGHEST)
        act = 0.5 * v * (1.0 + jnp.tanh(0.7978845608 * (v + 0.044715 * v * v * v)))
        act = act.astype(BF16)
        mix_buf[tp] = packed(act[:128], act[128:])

    def joined(ref):
        return jnp.concatenate([ref[s] for s in range(16)], axis=1)

    def up_part(c):
        if c == 0:
            loads[2].wait()
            loads[3].wait()
        piece = joined(rows_buf.at[c])
        hidden = (silu(dot(piece, wg[...])) * dot(piece, wu[...])).astype(BF16)
        hid_buf[c, 0, x] = hidden[: CHUNK // 2]
        hid_buf[c, 1, y] = hidden[CHUNK // 2 :]
        for turn in (0, 1):
            for side in (0, 1):
                hidden_copy(c, turn, side).start()

    def along(turn, d):
        return (ep, ((y + d) % 4) * 4 + x) if turn else (ep, y * 4 + (x + d) % 4)

    def hidden_copy(c, turn, side, passed=False):
        mine = y if turn else x
        back = 3 if side == 0 else 1
        ref = hid_buf.at[c, turn, (mine + back) % 4 if passed else mine]
        if passed:
            ref = ref.at[pl.ds(side * (CHUNK // 4), CHUNK // 4)]
        return pltpu.make_async_remote_copy(
            src_ref=ref,
            dst_ref=ref,
            send_sem=h_send.at[c, turn, 0],
            recv_sem=h_recv.at[c, turn, 2 if passed else side],
            device_id=along(turn, 1 if side == 0 else 3),
            device_id_type=MESH,
        )

    def weight_copy(turn, d, j):
        source = wd.at[j, (x + d) % 4] if turn else wd.at[(y + d) % 4, j]
        if d == 0:
            return pltpu.make_async_copy(source, wd_of.at[turn, 0, j], w_recv.at[turn, 0])
        return pltpu.make_async_remote_copy(
            src_ref=source,
            dst_ref=wd_of.at[turn, 4 - d, j],
            send_sem=w_send.at[turn, d],
            recv_sem=w_recv.at[turn, 4 - d],
            device_id=along(1 - turn, d),
            device_id_type=MESH,
        )

    def relay_copy(turn, side, j, passed):
        rows_here = pl.ds(side * 128, 128)
        source = wd.at[j, (x + 2) % 4, rows_here] if turn else wd.at[(y + 2) % 4, j, rows_here]
        hold = relay.at[turn, side, j]
        return pltpu.make_async_remote_copy(
            src_ref=hold if passed else source,
            dst_ref=wd_of.at[turn, 2, j, rows_here] if passed else hold,
            send_sem=w_send.at[turn, 0 if passed else 2],
            recv_sem=w_recv.at[turn, 2] if passed else relay_recv.at[turn, side, j],
            device_id=along(1 - turn, 3 if side else 1),
            device_id_type=MESH,
        )

    def send_weights(j):
        for turn in (0, 1):
            for d in (1, 3):
                weight_copy(turn, d, j).start()
        for turn in (0, 1):
            for side in (0, 1):
                relay_copy(turn, side, j, False).start()
            weight_copy(turn, 0, j).start()

    def relay_weights(j):
        for turn in (0, 1):
            for side in (0, 1):
                relay_copy(turn, side, j, False).wait_recv()
                relay_copy(turn, side, j, True).start()

    def wait_weights():
        for turn in (0, 1):
            for d in range(4):
                ref = wd_of.at[turn, d]
                pltpu.make_async_copy(ref, ref, w_recv.at[turn, d]).wait()

    def part_copy(c, turn, d):
        return pltpu.make_async_remote_copy(
            src_ref=part.at[c, turn, d],
            dst_ref=parts.at[c, turn, d],
            send_sem=h_send.at[c, turn, 1],
            recv_sem=h_recv.at[c, turn, 3],
            device_id=along(1 - turn, d),
            device_id_type=MESH,
        )

    def down_part(c, turn):
        ref = hid_buf.at[c, turn, 0]
        pltpu.make_async_copy(ref, ref, h_recv.at[c, turn, 2]).wait()
        hidden = jnp.concatenate([hid_buf[c, turn, i] for i in range(4)], axis=1)
        for pairs in ((1, 3), (2, 0)):
            weight = jnp.concatenate([wd_of[turn, d].reshape(1024, 128) for d in pairs], axis=1)
            sums = dot(hidden, weight).astype(BF16)
            for n, d in enumerate(pairs):
                value = sums[:, n * 128 : (n + 1) * 128]
                if d == 0:
                    parts[c, turn, 0] = value
                else:
                    part[c, turn, d] = value
                    part_copy(c, turn, d).start()

    def sum_part(c):
        for turn in (0, 1):
            ref = parts.at[c, turn, pl.ds(1, 3)]
            pltpu.make_async_copy(ref, ref, h_recv.at[c, turn, 3]).wait()
            total = sum(parts[c, turn, d].astype(F32) for d in range(4))
            start = c * CHUNK + turn * (CHUNK // 2)
            res[start : start + CHUNK // 2] = total.astype(BF16)
        for k in range(8 * c, 8 * c + 8):
            if k == 0:
                returned[0:CAP] = res[0:CAP]
                continue
            pltpu.make_async_remote_copy(
                src_ref=res.at[pl.ds(k * CAP, CAP)],
                dst_ref=returned.at[pl.ds(k * CAP, CAP)],
                send_sem=r_send,
                recv_sem=r_recv.at[c],
                device_id=(far(*SLOTS[k]), tp),
                device_id_type=MESH,
            ).start()

    def spread_out(buf, weight):
        height = buf.shape[1]
        low_half = iota((height, 128), 1) < 64
        total = jnp.zeros((2 * height, 128), F32)
        for s in range(16):
            block = buf[s]
            zero = jnp.zeros_like(block)
            both_rows = jnp.concatenate(
                [jnp.where(low_half, block, zero), jnp.where(low_half, zero, block)], axis=0
            )
            w = weight[s * 64 : (s + 1) * 64]
            total += dot(both_rows, jnp.concatenate([w, w], axis=0))
        return total

    def back_part():
        loads[14].wait()
        for c in range(CHUNKS):
            first, second = took(c)
            weighted = jnp.transpose(first * rw_ref[0:1, :] + second * rw_ref[1:2, :])
            rounded = weighted.astype(BF16)
            columns = slice(c * CHUNK, (c + 1) * CHUNK)
            back_hi[:, columns] = rounded
            back_lo[:, columns] = (weighted - rounded.astype(F32)).astype(BF16)

    def gain_part(c):
        with jax.named_scope(f"back{c}"):
            some = slice(CAP if c == 0 else c * CHUNK, (c + 1) * CHUNK)
            came = returned.at[some]
            pltpu.make_async_copy(came, came, r_recv.at[c]).wait()
        some = slice(c * CHUNK, (c + 1) * CHUNK)
        block = returned[some]
        return dot(back_hi[:, some], block) + dot(back_lo[:, some], block)

    gathers = {("shared", 0): shared, ("mixed", 0): mixed}
    for c in range(CHUNKS):
        gathers["rows", c] = rows[c]

    def begin(gather):
        for m in range(4):
            for turn in (0, 20):
                gather.copy(turn + m).start()

    loads[4].wait()
    send_weights(0)
    send_weights(1)
    shared_part()
    for c in (1, 2, 3):
        pack(c)
    down_first, here = True, set()
    for event in schedule():
        name, which = event[:2]
        if name == "message":
            _, gather, turn, m = event
            gathers[gather].copy(20 * turn + m).wait_recv()
            for following in passed_on(here, gather, turn, m):
                gathers[gather].copy(20 * turn + following).start()
        elif name == "leaves":
            gathers[which].leaves()
        elif name == "arrive":
            with jax.named_scope(f"arrive{which}"):
                rows_arrived(which)
            begin(rows[which])
            if which == 0:
                for c in (1, 2, 3):
                    send_chunk(c)
        elif name == "shared":
            begin(shared)
        elif name == "scan":
            with jax.named_scope("scan"):
                scan_part()
        elif name == "pair":
            pair_part()
        elif name == "back":
            with jax.named_scope("back"):
                back_part()
        elif name == "mixer":
            with jax.named_scope("mixer_part"):
                mixer_part()
            begin(mixed)
        elif name == "weights":
            send_weights(which)
        elif name == "relay":
            with jax.named_scope(f"relay{which}"):
                relay_weights(which)
        elif name == "up":
            with jax.named_scope(f"up{which}"):
                up_part(which)
        elif name == "near":
            with jax.named_scope(f"near{which}"):
                hidden_copy(*event[1:]).wait_recv()
                hidden_copy(*event[1:], passed=True).start()
        elif name == "down":
            if down_first:
                down_first = False
                with jax.named_scope("weights"):
                    wait_weights()
            with jax.named_scope(f"down{which}"):
                down_part(which, event[2])
        elif name == "sum":
            with jax.named_scope(f"sum{which}"):
                sum_part(which)
        elif name == "mix_out":
            with jax.named_scope("mix_out"):
                loads[6].wait()
                mix_ref[...] = spread_out(mix_buf, mixw).astype(BF16)
    loads[5].wait()
    common = spread_out(sh_buf, sd)
    for c in range(CHUNKS - 1):
        common += gain_part(c)

    with jax.named_scope("finish"):
        for gather in rows + [mixed, shared]:
            gather.finish()
        for turn in (0, 1):
            for c in range(CHUNKS):
                ref = hid_buf.at[c, turn, pl.ds(0, 3)]
                pltpu.make_async_copy(ref, ref, h_send.at[c, turn, 0]).wait()
                ref = part.at[c, turn, pl.ds(1, 3)]
                pltpu.make_async_copy(ref, ref, h_send.at[c, turn, 1]).wait()
            for d in range(4):
                ref = wd_of.at[turn, d]
                pltpu.make_async_copy(ref, ref, w_send.at[turn, d]).wait()
        to_partner().wait_send()
        for dz in range(1, 16):

            @pl.when(z + dz < 16)
            def _(dz=dz):
                to_chip(dz).wait_send()

    sent = outgoing.at[pl.ds(0, 31 * CAP)]
    pltpu.make_async_copy(sent, sent, z_send).wait()
    back = returned.at[pl.ds(0, 31 * CAP)]
    pltpu.make_async_copy(back, back, r_send).wait()
    common += gain_part(CHUNKS - 1)
    exp_ref[...] = common.astype(BF16)


def shards(
    mixer_input, log_step, decay_shift, input_map, readout, mixer_weight, expert_input,
    norm_gain, routes, route_weight, expert_switch_matrix, up_weight, down_weight,
    shared_gate, shared_up, shared_down,
):
    vmem = pl.BlockSpec(memory_space=pltpu.VMEM)
    hbm = pl.BlockSpec(memory_space=pltpu.HBM)
    V, DMA = pltpu.VMEM, pltpu.SemaphoreType.DMA
    return pl.pallas_call(
        body,
        out_shape=(
            jax.ShapeDtypeStruct((256, 128), BF16),
            jax.ShapeDtypeStruct((128, 128), BF16),
        ),
        in_specs=[pl.BlockSpec(memory_space=pltpu.SMEM)] + [hbm] * 15,
        out_specs=(vmem, vmem),
        scratch_shapes=[
            V((64, 256), BF16),
            V((4, 256), F32),
            V((128, 64), BF16),
            V((128, 64), F32),
            V((128, 2048), BF16),
            V((1, 2048), F32),
            V((2, 128), jnp.int32),
            V((2, 128), F32),
            V((1024, 128), BF16),
            V((2048, 256), BF16),
            V((2048, 256), BF16),
            V((4, 4, 256, 128), BF16),
            V((2, 4, 4, 256, 128), BF16),
            V((2, 2, 4, 128, 128), BF16),
            V((128, 2048), BF16),
            V((1024, 128), BF16),
            V((128, 2048), BF16),
            V((512, 128), BF16),
            V((128, 512), BF16),
            V((128, 512), BF16),
            V((CHUNKS, 16, CHUNK, 128), BF16),
            V((CHUNKS, 2, 4, CHUNK // 2, 256), BF16),
            V((CHUNKS, 2, 4, CHUNK // 2, 128), BF16),
            V((CHUNKS, 2, 4, CHUNK // 2, 128), BF16),
            V((512, 128), BF16),
            V((512, 128), BF16),
            V((16, 128, 128), BF16),
            V((16, 64, 128), BF16),
            V((2, 8, 128), F32),
            V((16, 8, 128), F32),
            V((2, 256, 128), F32),
            V((2, 256, 128), F32),
            V((2, 256, 128), F32),
            V((32, 256), F32),
            V((32, 256), F32),
            V((4, 8, 256), F32),
            DMA((15,)),
            DMA((CHUNKS + 2, 4)),
            DMA((CHUNKS + 2, 25)),
            DMA((CHUNKS, 2, 2)),
            DMA((CHUNKS, 2, 4)),
            DMA((2, 4)),
            DMA((2, 4)),
            DMA((2, 2, 4)),
            DMA,
            DMA((CHUNKS,)),
            DMA((16,)),
            DMA((16,)),
            DMA,
            DMA((CHUNKS,)),
        ],
        compiler_params=pltpu.CompilerParams(
            collective_id=0, has_side_effects=True, vmem_limit_bytes=67_043_328
        ),
    )(
        log_step,
        mixer_input.T,
        decay_shift.T,
        jnp.swapaxes(input_map, 2, 3).reshape(128, 64),
        readout.reshape(128, 64),
        expert_input,
        norm_gain.reshape(1, 2048),
        routes.T,
        route_weight.T,
        mixer_weight,
        expert_switch_matrix[0],
        up_weight[0],
        down_weight.reshape(4, 4, 256, 128),
        shared_gate.T,
        shared_up.T,
        shared_down,
    )


def solution(mesh):
    placed = (
        P("ep", "tp"),
        P("tp"),
        P("ep", "tp"),
        P(None, "tp", None, None),
        P(None, "tp", None, None),
        P(None, "tp"),
        P("ep", None),
        P(),
        P("ep", None),
        P("ep", None),
        P("ep", None, "tp"),
        P("ep", None, "tp"),
        P("ep", None, "tp"),
        P(None, "tp"),
        P(None, "tp"),
        P(None, "tp"),
    )
    return jax.shard_map(
        shards, mesh=mesh, in_specs=placed, out_specs=(P("ep", "tp"), P("ep", "tp")), check_vma=False
    )
```

```python
import heapq

import jax
import jax.numpy as jnp
from jax import lax
from jax.experimental import pallas as pl
from jax.experimental.pallas import tpu as pltpu
from jax.sharding import PartitionSpec as P

MESH = pl.DeviceIdType.MESH
F32 = jnp.float32
BF16 = jnp.bfloat16
HIGHEST = lax.Precision.HIGHEST

CHUNKS = 4
CHUNK = 128
CAP = 16
REACH = [0, 1, -1, 2, -4, 5, -5, 6, -6, 7, -7, 8, -2, 3, -3, 4]
SLOTS = [(dz, flip) for dz in REACH for flip in (0, 1)]


def dot(a, b, precision=None):
    return jnp.dot(a, b, preferred_element_type=F32, precision=precision)


def dot_nt(a, b, precision=None):
    return lax.dot_general(
        a, b, (((1,), (1,)), ((), ())), preferred_element_type=F32, precision=precision
    )


def dot_tn(a, b, precision=None):
    return lax.dot_general(
        a, b, (((0,), (0,)), ((), ())), preferred_element_type=F32, precision=precision
    )


def iota(shape, dim):
    return lax.broadcasted_iota(jnp.int32, shape, dim)


def put(ref, at, value):
    ref[0, at, :] = value[:, :128]
    ref[1, at, :] = value[:, 128:]


def got(ref, at):
    return jnp.concatenate([ref[0, at, :], ref[1, at, :]], axis=1)


THEN = {0: (4, 6, 7), 1: (5, 8, 9), 2: (10,), 3: (11,), 4: (12, 13), 5: (12, 13)}
THEN = {**THEN, 6: (14,), 7: (15,), 8: (16,), 9: (17,), 12: (18,), 13: (19,)}
PLACE = {**{m: m for m in range(10)}, 12: 21, 13: 22}
WHOLE = (0, 1, 2, 3, 6, 7, 8, 9, 12, 13)
RING = [0, 0, 1, 1, 0, 0] + [1] * 14
BACKWARD = [0, 1] * 10


def passed_on(here, gather, turn, m):
    here.add((gather, turn, m))
    if m in (4, 5) and (gather, turn, 9 - m) not in here:
        return ()
    return THEN[m]


def schedule(hop=2.3, rate=43000.0, later=(0.0, 7.0, 7.0, 14.0), mixer_at=27.0, trace=None):
    size = {("shared", 0): 16384, ("mixed", 0): 32768}
    rank = {("shared", 0): 0.5, ("mixed", 0): 3.5}
    for c in range(CHUNKS):
        size["rows", c] = 32768
        rank["rows", c] = c
    cost = {"scan": 2.2, "pair": 0.1, "back": 0.3, "mixer": 1.9, "mix_out": 0.6, "up": 0.47, "down": 0.35, "sum": 0.1}
    urgency = {"up": 1, "down": 1, "scan": 3, "pair": 3, "back": 4, "mixer": 3, "mix_out": 4, "sum": 0}
    now, free = 0.0, [0.5] * 4
    coming, ready, events = [], [], []
    ends = {gather: [] for gather in size}
    seen = {gather: 0 for gather in size}
    count, here, straight = {}, set(), {}

    def use(link, amount):
        nonlocal now
        now += 0.007
        free[link] = max(now, free[link]) + amount / rate
        return free[link] + hop

    def later_on(at, order, event):
        heapq.heappush(coming, (at, order, event))

    def send(gather, turn, m):
        link = (RING[m] ^ turn) * 2 + BACKWARD[m]
        at = use(link, size[gather] / (2 if m in WHOLE else 4))
        if m in THEN:
            later_on(at, rank[gather], ("message", gather, turn, m))
            return
        ends[gather].append(at)
        if len(ends[gather]) == 16:
            later_on(max(ends[gather]), rank[gather], ("leaves", gather))

    def begin(gather):
        for m in range(4):
            for turn in (0, 1):
                send(gather, turn, m)

    for c in range(CHUNKS):
        later_on(later[c], 0.0, ("arrive", c))
    for at, name in ((0.0, "shared"), (0.0, "scan"), (4.5, "pair"), (5.0, "back"), (mixer_at, "mixer")):
        later_on(at, 1.5, (name, 0))
    for at, event in ((0.015, ("weights", 2)), (2.4, ("relay", 0)), (2.4, ("relay", 1)), (3.0, ("weights", 3))):
        later_on(at, 9.0, event)
    while coming or ready:
        while coming and (coming[0][0] <= now or not ready):
            at, order, event = heapq.heappop(coming)
            now = max(now, at)
            heapq.heappush(ready, (urgency.get(event[0], 0), order, at, event))
        event = heapq.heappop(ready)[3]
        events.append(event)
        if trace is not None:
            trace[event] = now
        now += cost.get(event[0], 0.01)
        name, which = event[:2]
        if name in ("arrive", "shared", "mixer"):
            begin(({"arrive": "rows", "mixer": "mixed"}.get(name, name), which))
        elif name == "weights":
            for link in range(4):
                use(link, 65536)
            later_on(max(use(link, 32768) for link in range(4)), 9.0, ("relay", which))
        elif name == "relay":
            for link in range(4):
                use(link, 32768)
        elif name == "up":
            for turn in (0, 1):
                for side in (0, 1):
                    later_on(use(2 * turn + side, 32768), which, ("near", which, turn, side))
                if which == CHUNKS - 1:
                    use(2 * turn, 32768)
                    straight[turn] = use(2 * turn, 32768) + 0.8
        elif name == "near":
            turn, side = event[2:]
            at = straight[turn] if which == CHUNKS - 1 else use(2 * turn + side, 16384)
            count.setdefault((which, turn), []).append(at)
            if len(count[which, turn]) == 2:
                later_on(max(count[which, turn]), which, ("down", which, turn))
        elif name == "down":
            turn = 1 - event[2]
            at = max(use(2 * turn + side, 16384) for side in (0, 0, 1))
            count.setdefault(which, []).append(at)
            if len(count[which]) == 2:
                later_on(max(count[which]) + 0.5, which, ("sum", which))
        elif name in ("message", "leaves"):
            if name == "message":
                for m in passed_on(here, which, *event[2:]):
                    send(which, event[2], m)
            seen[which] += 1
            if seen[which] == 25:
                last = {"rows": "up", "mixed": "mix_out"}.get(which[0])
                if last:
                    heapq.heappush(ready, (urgency[last], rank[which], now, (last, which[1])))
    return events


class Gather:
    def __init__(self, buf, send, recv, number, place):
        self.buf, self.send, self.recv, self.number = buf, send, recv, number
        self.ep, self.y, self.x = place
        self.half = buf.shape[1] // 2
        self.plan = []
        for turned in (False, True):
            messages = [(0, 0, None, 0, 1), (0, 0, None, 0, -1), (0, 0, None, 1, 1), (0, 0, None, 1, -1)]
            messages += [(-1, 0, 0, 0, 1), (1, 0, 1, 0, -1)]
            messages += [(i, 0, None, 1, d) for i in (-1, 1) for d in (1, -1)]
            messages += [(0, -1, 0, 1, 1), (0, 1, 1, 1, -1)]
            messages += [(2, 0, None, 1, 1), (2, 0, None, 1, -1)]
            messages += [(i, -d, (1 - d) // 2, 1, d) for i in (-1, 1) for d in (1, -1)]
            messages += [(2, -1, 0, 1, 1), (2, 1, 1, 1, -1)]
            self.plan += [(turned, *m) for m in messages]

    def copy(self, m):
        turned, i, j, part, ring, step = self.plan[m]
        dy, dx = (i, j) if turned else (j, i)
        shard = ((self.y + dy + 4) % 4) * 4 + (self.x + dx + 4) % 4
        start, count = (self.half if turned else 0), self.half
        if part is not None:
            count = self.half // 2
            start += part * count
        along_y = (ring == 0) == turned
        ny = (self.y + step + 4) % 4 if along_y else self.y
        nx = self.x if along_y else (self.x + step + 4) % 4
        ref = self.buf.at[shard, pl.ds(start, count)]
        stage = sum(m % 20 >= first for first in (4, 12, 18))
        arrival = PLACE.get(m % 20)
        arrival = 20 if arrival is None else arrival + (2 if arrival > 20 else 10) * (m // 20)
        return pltpu.make_async_remote_copy(
            src_ref=ref,
            dst_ref=ref,
            send_sem=self.send.at[self.number, stage],
            recv_sem=self.recv.at[self.number, arrival],
            device_id=(self.ep, ny * 4 + nx),
            device_id_type=MESH,
        )

    def whole(self, count, sem):
        ref = self.buf.at[pl.ds(0, count)]
        pltpu.make_async_copy(ref, ref, sem).wait()

    def leaves(self):
        self.whole(4, self.recv.at[self.number, 20])

    def finish(self):
        for stage, count in enumerate((4, 6, 4, 1)):
            self.whole(count, self.send.at[self.number, stage])


def factors(log_step, state):
    step_rate = jnp.exp(log_step)
    frequency = jnp.pi * state.astype(F32)
    angle = step_rate * frequency
    turn_cosine = jnp.cos(angle)
    turn_sine = jnp.sin(angle)
    base = jnp.exp(-0.5 * step_rate)
    base_real = base * turn_cosine
    starting_quadrature = base * turn_sine
    inverse = 1.0 / (0.25 + frequency * frequency)
    lowered = base_real - 1.0
    inject_real = (-0.5 * lowered + starting_quadrature * frequency) * inverse
    inject_imaginary = (-0.5 * starting_quadrature - lowered * frequency) * inverse
    return (turn_cosine, turn_sine, inject_real, inject_imaginary, -0.5 * step_rate)


def body(
    step_ref, x_hbm, shift_hbm, imap_hbm, rout_hbm, e_hbm, gain_hbm, routes_hbm, rw_hbm,
    mixw_hbm, wg_hbm, wu_hbm, wd_hbm, sg_hbm, su_hbm, sd_hbm,
    mix_ref, exp_ref,
    x_ref, shift_ref, imap_ref, rout_ref, e_ref, gain_ref, routes_ref, rw_ref, mixw, wg, wu, wd, wd_of, relay, sgu, sd,
    normed, outgoing, back_hi, back_lo, rows_buf, hid_buf, part, parts, res, returned, mix_buf, sh_buf, pair, chips,
    push_r, push_i, mag, ph_r, ph_i, keep,
    load_sem, g_send, g_recv, h_send, h_recv, w_send, w_recv, relay_recv, z_send, z_recv, s_send, s_recv, r_send, r_recv,
    mix_val, exp_val, out_sem,
):
    ep, tp = lax.axis_index("ep"), lax.axis_index("tp")
    z, core = ep // 2, ep % 2
    y, x = tp // 4, tp % 4

    def out_copy(k):
        return pltpu.make_async_copy((mix_val, exp_val)[k], (mix_ref, exp_ref)[k], out_sem.at[k])

    def far(dz, flip):
        return ((z + dz + 16) % 16) * 2 + (core + flip) % 2

    chips[...] = jnp.zeros_like(chips)
    barrier = pltpu.get_barrier_semaphore()
    for dz, flip in SLOTS[1:]:
        pl.semaphore_signal(barrier, inc=1, device_id=(far(dz, flip), tp), device_id_type=MESH)
    for ny, nx in [(y, (x + d) % 4) for d in (1, 2, 3)] + [((y + d) % 4, x) for d in (1, 2, 3)]:
        pl.semaphore_signal(barrier, inc=1, device_id=(ep, ny * 4 + nx), device_id_type=MESH)

    loads = [
        pltpu.make_async_copy(src, dst, load_sem.at[k])
        for k, (src, dst) in enumerate(
            [(sg_hbm, sgu.at[0:64]), (su_hbm, sgu.at[64:128]), (wg_hbm, wg), (wu_hbm, wu),
             (wd_hbm, wd), (sd_hbm, sd), (mixw_hbm, mixw), (e_hbm, e_ref), (gain_hbm, gain_ref),
             (routes_hbm, routes_ref), (x_hbm, x_ref), (shift_hbm, shift_ref),
             (imap_hbm, imap_ref), (rout_hbm, rout_ref), (rw_hbm, rw_ref)]
        )
    ]
    for k in (7, 8, 9, 10, 11, 12, 13, 14, 0, 1, 2, 3, 4, 5, 6):
        loads[k].start()

    with jax.named_scope("load"):
        for k in (7, 8, 9):
            loads[k].wait()
    values = e_ref[...].astype(F32)
    scale = lax.rsqrt(jnp.mean(values * values, axis=-1, keepdims=True) + 1e-06)
    normed[...] = (values * scale * gain_ref[...]).astype(BF16)
    expert = iota((32, 128), 0)
    named = [(routes_ref[k : k + 1, :] == expert).astype(F32) for k in (0, 1)]
    earlier = (iota((128, 128), 0) < iota((128, 128), 1)).astype(BF16)
    before = dot((named[0] + named[1]).astype(BF16), earlier)
    target = []
    for k in (0, 1):
        rank = jnp.sum(named[k] * before, axis=0, keepdims=True).astype(jnp.int32)
        route = routes_ref[k : k + 1, :]
        away = (z + 16 - (route >> 1)) & 15
        turn = jnp.zeros_like(route)
        for i, dz in enumerate(REACH):
            turn = jnp.where(away == dz % 16, i, turn)
        target.append((turn * 2 + ((route + core) & 1)) * CAP + rank)
    own = normed[:, pl.ds(pl.multiple_of(tp * 128, 128), 128)]

    def took(c):
        slot = iota((CHUNK, 128), 0) + c * CHUNK
        return [(target[k] == slot).astype(F32) for k in (0, 1)]

    def pack(c):
        first, second = took(c)
        outgoing[c * CHUNK : (c + 1) * CHUNK] = dot((first + second).astype(BF16), own).astype(BF16)

    pack(0)
    with jax.named_scope("enter"):
        pl.semaphore_wait(barrier, len(SLOTS) - 1 + 6)

    def send_chunk(c):
        for k in range(max(1, 8 * c), 8 * c + 8):
            dz, flip = SLOTS[k]
            pltpu.make_async_remote_copy(
                src_ref=outgoing.at[pl.ds(k * CAP, CAP)],
                dst_ref=rows_buf.at[c, tp, pl.ds((k - 8 * c) * CAP, CAP)],
                send_sem=z_send,
                recv_sem=z_recv.at[c],
                device_id=(far(-dz, flip), tp),
                device_id_type=MESH,
            ).start()

    send_chunk(0)
    rows_buf[0, tp, 0:CAP] = outgoing[0:CAP]

    def rows_arrived(c):
        if c == 0:
            ref = rows_buf.at[0, tp, pl.ds(CAP, CHUNK - CAP)]
        else:
            ref = rows_buf.at[c, tp]
        pltpu.make_async_copy(ref, ref, z_recv.at[c]).wait()

    def to_partner():
        return pltpu.make_async_remote_copy(
            src_ref=pair.at[core],
            dst_ref=pair.at[core],
            send_sem=s_send.at[0],
            recv_sem=s_recv.at[0],
            device_id=(far(0, 1), tp),
            device_id_type=MESH,
        )

    def to_chip(dz):
        return pltpu.make_async_remote_copy(
            src_ref=chips.at[z],
            dst_ref=chips.at[z],
            send_sem=s_send.at[dz],
            recv_sem=s_recv.at[dz],
            device_id=(far(dz, 0), tp),
            device_id_type=MESH,
        )

    def parts_of(ref, i):
        return [ref[i, 2 * n : 2 * n + 2, :] for n in range(4)]

    def after(early_r, early_i, late):
        a_r, a_i, c_r, c_i = late
        return a_r * early_r - a_i * early_i + c_r, a_r * early_i + a_i * early_r + c_i

    def pair_part():
        to_partner().wait_recv()
        first, second = parts_of(pair, 0), parts_of(pair, 1)
        a_r, a_i = first[0] * second[0] - first[1] * second[1], first[0] * second[1] + first[1] * second[0]
        c_r, c_i = after(first[2], first[3], second)
        for n, part in enumerate((a_r, a_i, c_r, c_i)):
            chips[z, 2 * n : 2 * n + 2, :] = part
        for dz in range(1, 16):

            @pl.when(z + dz < 16)
            def _(dz=dz):
                to_chip(dz).start()

    def scan_part():
        with jax.named_scope("load2"):
            for k in (10, 11, 12):
                loads[k].wait()
        group = iota((1, 256), 1) // 64
        log_step = jnp.where(group == 0, step_ref[0], step_ref[1])
        log_step = jnp.where(group == 2, step_ref[2], log_step)
        log_step = jnp.where(group == 3, step_ref[3], log_step)
        cosine, sine, inj_r, inj_i, low = factors(log_step, iota((1, 256), 1) % 64)
        spread = (iota((64, 256), 1) % 64 == iota((64, 256), 0)).astype(BF16)
        mine = iota((64, 256), 0) // 16 == iota((64, 256), 1) // 64
        drive_r, drive_i = [
            dot_tn(
                x_ref[...],
                jnp.where(mine, dot(imap_ref[64 * c : 64 * c + 64, :], spread), 0.0).astype(BF16),
            )
            for c in (0, 1)
        ]
        every = slice(None)
        put(push_r, every, inj_r * drive_r - inj_i * drive_i)
        put(push_i, every, inj_r * drive_i + inj_i * drive_r)
        of_group = (iota((4, 256), 1) // 64 == iota((4, 256), 0)).astype(F32)
        put(mag, every, jnp.exp(low + dot_tn(shift_ref[...], of_group, HIGHEST)))
        state_r, state_i = jnp.zeros((8, 256), F32), jnp.zeros((8, 256), F32)
        total = jnp.ones((8, 256), F32)
        turn_r, turn_i = jnp.ones((1, 256), F32), jnp.zeros((1, 256), F32)
        for j in range(32):
            at = pl.ds(j, 8, stride=32)
            m = got(mag, at)
            d_r, d_i = m * cosine, m * sine
            state_r, state_i = (
                d_r * state_r - d_i * state_i + got(push_r, at),
                d_r * state_i + d_i * state_r + got(push_i, at),
            )
            total = total * m
            turn_r, turn_i = turn_r * cosine - turn_i * sine, turn_r * sine + turn_i * cosine
            put(push_r, at, state_r)
            put(push_i, at, state_i)
            put(mag, at, total)
            ph_r[j : j + 1, :] = turn_r
            ph_i[j : j + 1, :] = turn_i
        all_r, all_i = total * turn_r, total * turn_i
        c_r, c_i = jnp.zeros((1, 256), F32), jnp.zeros((1, 256), F32)
        t_r, t_i = jnp.ones((1, 256), F32), jnp.zeros((1, 256), F32)
        for s in range(8):
            for n, part in enumerate((t_r, t_i, c_r, c_i)):
                keep[n, s : s + 1, :] = part
            a_r, a_i = all_r[s : s + 1], all_i[s : s + 1]
            c_r, c_i = (
                a_r * c_r - a_i * c_i + state_r[s : s + 1],
                a_r * c_i + a_i * c_r + state_i[s : s + 1],
            )
            t_r, t_i = a_r * t_r - a_i * t_i, a_r * t_i + a_i * t_r
        for n, part in enumerate((t_r, t_i, c_r, c_i)):
            pair[core, 2 * n : 2 * n + 1, :] = part[:, :128]
            pair[core, 2 * n + 1 : 2 * n + 2, :] = part[:, 128:]
        to_partner().start()

    place = (ep, y, x)
    rows = [Gather(rows_buf.at[c], g_send, g_recv, c, place) for c in range(CHUNKS)]
    mixed = Gather(mix_buf, g_send, g_recv, CHUNKS, place)
    shared = Gather(sh_buf, g_send, g_recv, CHUNKS + 1, place)

    def packed(top, bottom):
        first = (iota((64, 128), 1) == iota((64, 128), 0)).astype(BF16)
        second = (iota((64, 128), 1) == iota((64, 128), 0) + 64).astype(BF16)
        return (dot(top, first) + dot(bottom, second)).astype(BF16)

    def silu(v):
        return v / (1.0 + jnp.exp(-v))

    def shared_part():
        loads[0].wait()
        loads[1].wait()
        both_sums = dot_nt(normed[...], sgu[...])
        hidden = (silu(both_sums[:, :64]) * both_sums[:, 64:]).astype(BF16)
        sh_buf[tp] = packed(hidden[:64], hidden[64:])

    def mixer_part():
        with jax.named_scope("sums"):
            for dz in range(1, 16):

                @pl.when(z - dz >= 0)
                def _(dz=dz):
                    to_chip(dz).wait_recv()

        in_r, in_i = jnp.zeros((2, 128), F32), jnp.zeros((2, 128), F32)
        for i in range(15):
            n_r, n_i = after(in_r, in_i, parts_of(chips, i))
            in_r, in_i = jnp.where(i < z, n_r, in_r), jnp.where(i < z, n_i, in_i)
        n_r, n_i = after(in_r, in_i, parts_of(pair, 0))
        in_r, in_i = jnp.where(core == 1, n_r, in_r), jnp.where(core == 1, n_i, in_i)
        in_r = jnp.concatenate([in_r[0:1], in_r[1:2]], axis=1)
        in_i = jnp.concatenate([in_i[0:1], in_i[1:2]], axis=1)
        k_r, k_i = keep[0], keep[1]
        car_r = k_r * in_r - k_i * in_i + keep[2]
        car_i = k_r * in_i + k_i * in_r + keep[3]
        for j in range(32):
            at = pl.ds(j, 8, stride=32)
            p_r, p_i, m = ph_r[j : j + 1, :], ph_i[j : j + 1, :], got(mag, at)
            put(push_r, at, got(push_r, at) + m * (p_r * car_r - p_i * car_i))
            put(push_i, at, got(push_i, at) + m * (p_r * car_i + p_i * car_r))
        loads[13].wait()
        spread = (iota((64, 256), 1) % 64 == iota((64, 256), 0)).astype(F32)
        mine = iota((64, 256), 0) // 16 == iota((64, 256), 1) // 64
        out_r = jnp.where(mine, dot(rout_ref[0:64, :], spread, HIGHEST), 0.0)
        out_i = jnp.where(mine, dot(rout_ref[64:128, :], spread, HIGHEST), 0.0)
        every = slice(None)
        v = dot_nt(got(push_r, every), out_r, HIGHEST) - dot_nt(got(push_i, every), out_i, HIGHEST)
        act = 0.5 * v * (1.0 + jnp.tanh(0.7978845608 * (v + 0.044715 * v * v * v)))
        act = act.astype(BF16)
        mix_buf[tp] = packed(act[:128], act[128:])

    def joined(ref):
        return jnp.concatenate([ref[s] for s in range(16)], axis=1)

    def up_part(c):
        if c == 0:
            loads[2].wait()
            loads[3].wait()
        piece = joined(rows_buf.at[c])
        hidden = (silu(dot(piece, wg[...])) * dot(piece, wu[...])).astype(BF16)
        hid_buf[c, 0, x] = hidden[: CHUNK // 2]
        hid_buf[c, 1, y] = hidden[CHUNK // 2 :]
        for turn in (0, 1):
            for side in (0, 1):
                hidden_copy(c, turn, side).start()
            if c == CHUNKS - 1:
                straight_copy(c, turn).start()

    def straight_copy(c, turn):
        ref = hid_buf.at[c, turn, y if turn else x]
        return pltpu.make_async_remote_copy(
            src_ref=ref,
            dst_ref=ref,
            send_sem=h_send.at[c, turn, 0],
            recv_sem=h_recv.at[c, turn, 2],
            device_id=along(turn, 2),
            device_id_type=MESH,
        )

    def along(turn, d):
        return (ep, ((y + d) % 4) * 4 + x) if turn else (ep, y * 4 + (x + d) % 4)

    def hidden_copy(c, turn, side, passed=False):
        mine = y if turn else x
        back = 3 if side == 0 else 1
        ref = hid_buf.at[c, turn, (mine + back) % 4 if passed else mine]
        if passed:
            ref = ref.at[pl.ds(side * (CHUNK // 4), CHUNK // 4)]
        return pltpu.make_async_remote_copy(
            src_ref=ref,
            dst_ref=ref,
            send_sem=h_send.at[c, turn, 0],
            recv_sem=h_recv.at[c, turn, 2 if passed else side],
            device_id=along(turn, 1 if side == 0 else 3),
            device_id_type=MESH,
        )

    def weight_copy(turn, d, j):
        source = wd.at[j, (x + d) % 4] if turn else wd.at[(y + d) % 4, j]
        if d == 0:
            return pltpu.make_async_copy(source, wd_of.at[turn, 0, j], w_recv.at[turn, 0])
        return pltpu.make_async_remote_copy(
            src_ref=source,
            dst_ref=wd_of.at[turn, 4 - d, j],
            send_sem=w_send.at[turn, d],
            recv_sem=w_recv.at[turn, 4 - d],
            device_id=along(1 - turn, d),
            device_id_type=MESH,
        )

    def relay_copy(turn, side, j, passed):
        rows_here = pl.ds(side * 128, 128)
        source = wd.at[j, (x + 2) % 4, rows_here] if turn else wd.at[(y + 2) % 4, j, rows_here]
        hold = relay.at[turn, side, j]
        return pltpu.make_async_remote_copy(
            src_ref=hold if passed else source,
            dst_ref=wd_of.at[turn, 2, j, rows_here] if passed else hold,
            send_sem=w_send.at[turn, 0 if passed else 2],
            recv_sem=w_recv.at[turn, 2] if passed else relay_recv.at[turn, side, j],
            device_id=along(1 - turn, 3 if side else 1),
            device_id_type=MESH,
        )

    def send_weights(j):
        for turn in (0, 1):
            for d in (1, 3):
                weight_copy(turn, d, j).start()
        for turn in (0, 1):
            for side in (0, 1):
                relay_copy(turn, side, j, False).start()
            weight_copy(turn, 0, j).start()

    def relay_weights(j):
        for turn in (0, 1):
            for side in (0, 1):
                relay_copy(turn, side, j, False).wait_recv()
                relay_copy(turn, side, j, True).start()

    def wait_weights():
        for turn in (0, 1):
            for d in range(4):
                ref = wd_of.at[turn, d]
                pltpu.make_async_copy(ref, ref, w_recv.at[turn, d]).wait()

    def part_copy(c, turn, d):
        return pltpu.make_async_remote_copy(
            src_ref=part.at[c, turn, d],
            dst_ref=parts.at[c, turn, d],
            send_sem=h_send.at[c, turn, 1],
            recv_sem=h_recv.at[c, turn, 3],
            device_id=along(1 - turn, d),
            device_id_type=MESH,
        )

    def down_part(c, turn):
        ref = hid_buf.at[c, turn, 0]
        pltpu.make_async_copy(ref, ref, h_recv.at[c, turn, 2]).wait()
        hidden = jnp.concatenate([hid_buf[c, turn, i] for i in range(4)], axis=1)
        for pairs in ((1, 3), (2, 0)):
            weight = jnp.concatenate([wd_of[turn, d].reshape(1024, 128) for d in pairs], axis=1)
            sums = dot(hidden, weight).astype(BF16)
            for n, d in enumerate(pairs):
                value = sums[:, n * 128 : (n + 1) * 128]
                if d == 0:
                    parts[c, turn, 0] = value
                else:
                    part[c, turn, d] = value
                    part_copy(c, turn, d).start()

    def sum_part(c):
        for turn in (0, 1):
            ref = parts.at[c, turn, pl.ds(1, 3)]
            pltpu.make_async_copy(ref, ref, h_recv.at[c, turn, 3]).wait()
            total = sum(parts[c, turn, d].astype(F32) for d in range(4))
            start = c * CHUNK + turn * (CHUNK // 2)
            res[start : start + CHUNK // 2] = total.astype(BF16)
        for k in range(8 * c, 8 * c + 8):
            if k == 0:
                returned[0:CAP] = res[0:CAP]
                continue
            pltpu.make_async_remote_copy(
                src_ref=res.at[pl.ds(k * CAP, CAP)],
                dst_ref=returned.at[pl.ds(k * CAP, CAP)],
                send_sem=r_send,
                recv_sem=r_recv.at[c],
                device_id=(far(*SLOTS[k]), tp),
                device_id_type=MESH,
            ).start()

    def spread_out(buf, weight):
        height = buf.shape[1]
        low_half = iota((height, 128), 1) < 64
        total = jnp.zeros((2 * height, 128), F32)
        for s in range(16):
            block = buf[s]
            zero = jnp.zeros_like(block)
            both_rows = jnp.concatenate(
                [jnp.where(low_half, block, zero), jnp.where(low_half, zero, block)], axis=0
            )
            w = weight[s * 64 : (s + 1) * 64]
            total += dot(both_rows, jnp.concatenate([w, w], axis=0))
        return total

    def back_part():
        loads[14].wait()
        for c in range(CHUNKS):
            first, second = took(c)
            weighted = jnp.transpose(first * rw_ref[0:1, :] + second * rw_ref[1:2, :])
            rounded = weighted.astype(BF16)
            columns = slice(c * CHUNK, (c + 1) * CHUNK)
            back_hi[:, columns] = rounded
            back_lo[:, columns] = (weighted - rounded.astype(F32)).astype(BF16)

    def gain_part(c):
        with jax.named_scope(f"back{c}"):
            some = slice(CAP if c == 0 else c * CHUNK, (c + 1) * CHUNK)
            came = returned.at[some]
            pltpu.make_async_copy(came, came, r_recv.at[c]).wait()
        some = slice(c * CHUNK, (c + 1) * CHUNK)
        block = returned[some]
        return dot(back_hi[:, some], block) + dot(back_lo[:, some], block)

    gathers = {("shared", 0): shared, ("mixed", 0): mixed}
    for c in range(CHUNKS):
        gathers["rows", c] = rows[c]

    def begin(gather):
        for m in range(4):
            for turn in (0, 20):
                gather.copy(turn + m).start()

    loads[4].wait()
    send_weights(0)
    send_weights(1)
    shared_part()
    for c in (1, 2, 3):
        pack(c)
    down_first, here = True, set()
    for event in schedule():
        name, which = event[:2]
        if name == "message":
            _, gather, turn, m = event
            gathers[gather].copy(20 * turn + m).wait_recv()
            for following in passed_on(here, gather, turn, m):
                gathers[gather].copy(20 * turn + following).start()
        elif name == "leaves":
            gathers[which].leaves()
        elif name == "arrive":
            with jax.named_scope(f"arrive{which}"):
                rows_arrived(which)
            begin(rows[which])
            if which == 0:
                for c in (1, 2, 3):
                    send_chunk(c)
        elif name == "shared":
            begin(shared)
        elif name == "scan":
            with jax.named_scope("scan"):
                scan_part()
        elif name == "pair":
            pair_part()
        elif name == "back":
            with jax.named_scope("back"):
                back_part()
        elif name == "mixer":
            with jax.named_scope("mixer_part"):
                mixer_part()
            begin(mixed)
        elif name == "weights":
            send_weights(which)
        elif name == "relay":
            with jax.named_scope(f"relay{which}"):
                relay_weights(which)
        elif name == "up":
            with jax.named_scope(f"up{which}"):
                up_part(which)
        elif name == "near":
            with jax.named_scope(f"near{which}"):
                hidden_copy(*event[1:]).wait_recv()
                if which < CHUNKS - 1:
                    hidden_copy(*event[1:], passed=True).start()
        elif name == "down":
            if down_first:
                down_first = False
                with jax.named_scope("weights"):
                    wait_weights()
            with jax.named_scope(f"down{which}"):
                down_part(which, event[2])
        elif name == "sum":
            with jax.named_scope(f"sum{which}"):
                sum_part(which)
        elif name == "mix_out":
            with jax.named_scope("mix_out"):
                loads[6].wait()
                mix_val[...] = spread_out(mix_buf, mixw).astype(BF16)
                out_copy(0).start()
    loads[5].wait()
    common = spread_out(sh_buf, sd)
    for c in range(CHUNKS - 1):
        common += gain_part(c)

    with jax.named_scope("finish"):
        for gather in rows + [mixed, shared]:
            gather.finish()
        for turn in (0, 1):
            for c in range(CHUNKS):
                ref = hid_buf.at[c, turn, pl.ds(0, 3)]
                pltpu.make_async_copy(ref, ref, h_send.at[c, turn, 0]).wait()
                ref = part.at[c, turn, pl.ds(1, 3)]
                pltpu.make_async_copy(ref, ref, h_send.at[c, turn, 1]).wait()
            for d in range(4):
                ref = wd_of.at[turn, d]
                pltpu.make_async_copy(ref, ref, w_send.at[turn, d]).wait()
        to_partner().wait_send()
        for dz in range(1, 16):

            @pl.when(z + dz < 16)
            def _(dz=dz):
                to_chip(dz).wait_send()

    sent = outgoing.at[pl.ds(0, 31 * CAP)]
    pltpu.make_async_copy(sent, sent, z_send).wait()
    back = returned.at[pl.ds(0, 31 * CAP)]
    pltpu.make_async_copy(back, back, r_send).wait()
    common += gain_part(CHUNKS - 1)
    exp_val[...] = common.astype(BF16)
    out_copy(1).start()
    out_copy(0).wait()
    out_copy(1).wait()


def shards(
    mixer_input, log_step, decay_shift, input_map, readout, mixer_weight, expert_input,
    norm_gain, routes, route_weight, expert_switch_matrix, up_weight, down_weight,
    shared_gate, shared_up, shared_down,
):
    hbm = pl.BlockSpec(memory_space=pltpu.HBM)
    V, DMA = pltpu.VMEM, pltpu.SemaphoreType.DMA
    return pl.pallas_call(
        body,
        out_shape=(
            jax.ShapeDtypeStruct((256, 128), BF16),
            jax.ShapeDtypeStruct((128, 128), BF16),
        ),
        in_specs=[pl.BlockSpec(memory_space=pltpu.SMEM)] + [hbm] * 15,
        out_specs=(hbm, hbm),
        scratch_shapes=[
            V((64, 256), BF16),
            V((4, 256), F32),
            V((128, 64), BF16),
            V((128, 64), F32),
            V((128, 2048), BF16),
            V((1, 2048), F32),
            V((2, 128), jnp.int32),
            V((2, 128), F32),
            V((1024, 128), BF16),
            V((2048, 256), BF16),
            V((2048, 256), BF16),
            V((4, 4, 256, 128), BF16),
            V((2, 4, 4, 256, 128), BF16),
            V((2, 2, 4, 128, 128), BF16),
            V((128, 2048), BF16),
            V((1024, 128), BF16),
            V((128, 2048), BF16),
            V((512, 128), BF16),
            V((128, 512), BF16),
            V((128, 512), BF16),
            V((CHUNKS, 16, CHUNK, 128), BF16),
            V((CHUNKS, 2, 4, CHUNK // 2, 256), BF16),
            V((CHUNKS, 2, 4, CHUNK // 2, 128), BF16),
            V((CHUNKS, 2, 4, CHUNK // 2, 128), BF16),
            V((512, 128), BF16),
            V((512, 128), BF16),
            V((16, 128, 128), BF16),
            V((16, 64, 128), BF16),
            V((2, 8, 128), F32),
            V((16, 8, 128), F32),
            V((2, 256, 128), F32),
            V((2, 256, 128), F32),
            V((2, 256, 128), F32),
            V((32, 256), F32),
            V((32, 256), F32),
            V((4, 8, 256), F32),
            DMA((15,)),
            DMA((CHUNKS + 2, 4)),
            DMA((CHUNKS + 2, 25)),
            DMA((CHUNKS, 2, 2)),
            DMA((CHUNKS, 2, 4)),
            DMA((2, 4)),
            DMA((2, 4)),
            DMA((2, 2, 4)),
            DMA,
            DMA((CHUNKS,)),
            DMA((16,)),
            DMA((16,)),
            DMA,
            DMA((CHUNKS,)),
            V((256, 128), BF16),
            V((128, 128), BF16),
            DMA((2,)),
        ],
        compiler_params=pltpu.CompilerParams(
            collective_id=0, has_side_effects=True, vmem_limit_bytes=67_043_328
        ),
    )(
        log_step,
        mixer_input.T,
        decay_shift.T,
        jnp.swapaxes(input_map, 2, 3).reshape(128, 64),
        readout.reshape(128, 64),
        expert_input,
        norm_gain.reshape(1, 2048),
        routes.T,
        route_weight.T,
        mixer_weight,
        expert_switch_matrix[0],
        up_weight[0],
        down_weight.reshape(4, 4, 256, 128),
        shared_gate.T,
        shared_up.T,
        shared_down,
    )


def solution(mesh):
    placed = (
        P("ep", "tp"),
        P("tp"),
        P("ep", "tp"),
        P(None, "tp", None, None),
        P(None, "tp", None, None),
        P(None, "tp"),
        P("ep", None),
        P(),
        P("ep", None),
        P("ep", None),
        P("ep", None, "tp"),
        P("ep", None, "tp"),
        P("ep", None, "tp"),
        P(None, "tp"),
        P(None, "tp"),
        P(None, "tp"),
    )
    return jax.shard_map(
        shards, mesh=mesh, in_specs=placed, out_specs=(P("ep", "tp"), P("ep", "tp")), check_vma=False
    )
```
